32 devices in a mesh: rep: 2 (over y), fs: 4 (over z), tp: 4 (over x, core).
Axes of the slice: x: 2, y: 2, z: 4, core: 2. Of those that a mesh axis runs over, the one named last changes fastest.
Arguments:
- activations: bfloat16 [2048, 4096], P(None, ('rep', 'fs')), may hold values from -60 to 60
- w_mix_in: bfloat16 [2048, 1024], P('fs', 'tp'), may hold values from -0.125 to 0.125
- w_mix_out: bfloat16 [2048, 1024], P('fs', 'tp'), may hold values from -0.1875 to 0.1875
- w_gate: bfloat16 [2048, 2816], P('fs', 'tp'), may hold values from -0.125 to 0.125
- w_up: bfloat16 [2048, 2816], P('fs', 'tp'), may hold values from -0.125 to 0.125
- w_down: bfloat16 [2048, 2816], P('fs', 'tp'), may hold values from -0.109375 to 0.109375
- pool_scale: float32 [1024], replicated, may hold values from 0.1 to 1.9
- gain_mix: float32 [2048], replicated, may hold values from 0.1 to 1.9
- gain_ffn: float32 [2048], replicated, may hold values from 0.1 to 1.9
- gain_out: float32 [2048], replicated, may hold values from 0.1 to 1.9
Outputs:
- normalized: bfloat16 [2048, 4096], P('tp', ('rep', 'fs'))
The draws below stay inside these ranges and needn't reach their ends.
All inputs are finite; a program needn't handle non-finite values.
Results may differ from the reference program's by a relative error of at most 0.014.
Values may be sent and summed in bfloat16 or wider, within the bound.
A program may use at most 64 MiB of HBM per device.

```python
import jax
import jax.numpy as jnp
from jax import lax

D = 2048
BRANCH = 1024
FF = 2816
POOL_GROUP = 256
SEQ_LEN = 256
TOKENS = 4096
N_TP = 4


def draw_activations(key, part):
    key_rough, key_noise = jax.random.split(key, 2)
    feature_place = jnp.arange(D, dtype=jnp.float32)[:, None] / D
    rough = jax.random.uniform(key_rough, (D, 1), jnp.float32, -0.3, 0.3)
    feature_scale = 0.5 * jnp.exp(jnp.log(8.0) * feature_place + rough)
    values = jnp.clip(jax.random.normal(key_noise, (D, TOKENS), jnp.float32), -6.0, 6.0)
    return jnp.clip(values * feature_scale, -60.0, 60.0).astype(jnp.bfloat16)


def levels(own_key, shape, shards, smallest, top_value):
    def one(axis_at, blocks):
        draws = jax.random.uniform(jax.random.fold_in(jax.random.fold_in(own_key, 6), axis_at), (blocks,), jnp.float32, smallest / len(shards), top_value / len(shards))
        return jnp.repeat(jnp.exp(draws), shape[axis_at] // blocks).reshape((-1,) + (1,) * (len(shape) - axis_at - 1))

    gain = one(*shards[0])
    for cut in shards[1:]:
        gain = gain * one(*cut)
    return gain


def gaussian(rng, shape, scale, reach, shards=(), kind=jnp.bfloat16):
    drawn = scale * jax.random.normal(rng, shape, jnp.float32)
    if shards:
        drawn = drawn * levels(rng, shape, shards, -0.22, 0.18)
    return jnp.clip(drawn, -reach, reach).astype(kind)


def setup_inputs(seed: int = 0) -> dict:
    key_list = jax.random.split(jax.random.key(seed), 11)
    activations = draw_activations(jax.random.fold_in(key_list[10], 71), 0)
    w_mix_in = gaussian(key_list[1], (D, BRANCH), D ** -0.5, 0.125, ((0, 4), (1, 4)))
    w_mix_out = gaussian(key_list[2], (D, BRANCH), BRANCH ** -0.5, 0.1875, ((0, 4), (1, 4)))
    w_gate = gaussian(key_list[3], (D, FF), D ** -0.5, 0.125, ((0, 4), (1, 4)))
    w_up = gaussian(key_list[4], (D, FF), D ** -0.5, 0.125, ((0, 4), (1, 4)))
    w_down = gaussian(key_list[5], (D, FF), FF ** -0.5, 0.109375, ((0, 4), (1, 4)))
    pool_scale = jnp.clip(1.0 + 0.18 * jax.random.normal(key_list[6], (BRANCH,), jnp.float32), 0.1, 1.9)
    gain_mix = jnp.clip(1.0 + 0.18 * jax.random.normal(key_list[7], (D,), jnp.float32), 0.1, 1.9)
    gain_ffn = jnp.clip(1.0 + 0.18 * jax.random.normal(key_list[8], (D,), jnp.float32), 0.1, 1.9)
    gain_out = jnp.clip(1.0 + 0.18 * jax.random.normal(key_list[9], (D,), jnp.float32), 0.1, 1.9)
    return {"activations": activations, "w_mix_in": w_mix_in, "w_mix_out": w_mix_out, "w_gate": w_gate, "w_up": w_up, "w_down": w_down, "pool_scale": pool_scale, "gain_mix": gain_mix, "gain_ffn": gain_ffn, "gain_out": gain_out}


EPS = 1e-06
WINDOWS = (2, 4, 8, 16)

def rms_factor(stream):
    return lax.rsqrt(lax.optimization_barrier(jnp.mean(stream * stream, axis=0, keepdims=True)) + EPS)

def pool_tokens(inputs, group_of):
    channels = inputs.shape[0]
    values = inputs.astype(jnp.float32).reshape(channels, -1, SEQ_LEN)
    sequences = values.shape[1]
    running = jnp.concatenate([jnp.zeros((channels, sequences, 1), jnp.float32), jnp.cumsum(values, axis=-1)], axis=-1)
    places = jnp.arange(SEQ_LEN, dtype=jnp.int32)
    pooled_sum = jnp.zeros_like(values)
    for group_id, window in enumerate(WINDOWS):
        behind = window // 2
        onward = window - behind
        upper_sum = jnp.concatenate([running, jnp.repeat(running[..., -1:], onward, axis=-1)], axis=-1)[..., onward:onward + SEQ_LEN]
        lower_sum = jnp.concatenate([jnp.zeros((channels, sequences, behind), jnp.float32), running], axis=-1)[..., :SEQ_LEN]
        counts = (jnp.minimum(places + onward, SEQ_LEN) - jnp.maximum(places - behind, 0)).astype(jnp.float32)
        window_mean = (upper_sum - lower_sum) / counts
        pooled_sum = pooled_sum + jnp.where((group_of == group_id)[:, None, None], window_mean, 0.0)
    return (pooled_sum - values).reshape(channels, -1)

def block_sum(weights, acts, blocks):
    width = acts.shape[0] // blocks
    stacked_weights = jnp.transpose(weights.reshape(weights.shape[0], blocks, width), (1, 0, 2))
    stacked_acts = acts.reshape(blocks, width, acts.shape[1])

    def add_block(carry, pair):
        term = jnp.dot(pair[0], pair[1], preferred_element_type=jnp.float32).astype(jnp.bfloat16)
        term = lax.optimization_barrier(term)
        return (carry + term.astype(jnp.float32), None)
    start = jnp.zeros((weights.shape[0], acts.shape[1]), jnp.float32)
    total, _ = lax.scan(add_block, start, (stacked_weights, stacked_acts))
    return total

def reference(activations, w_mix_in, w_mix_out, w_gate, w_up, w_down, pool_scale, gain_mix, gain_ffn, gain_out):
    stream = activations.astype(jnp.float32)
    normed = (stream * rms_factor(stream) * gain_mix[:, None]).astype(jnp.bfloat16)
    inputs = jnp.dot(w_mix_in.T, normed, preferred_element_type=jnp.float32).astype(jnp.bfloat16)
    group_of = (jnp.arange(BRANCH, dtype=jnp.int32) // POOL_GROUP).astype(jnp.int32)
    pooled = (pool_tokens(inputs, group_of) * pool_scale[:, None]).astype(jnp.bfloat16)
    mixed = block_sum(w_mix_out, pooled, N_TP)
    after_mix = lax.optimization_barrier((stream + mixed).astype(jnp.bfloat16)).astype(jnp.float32)
    normed_two = (after_mix * rms_factor(after_mix) * gain_ffn[:, None]).astype(jnp.bfloat16)
    gate = jnp.dot(w_gate.T, normed_two, preferred_element_type=jnp.float32)
    upward = jnp.dot(w_up.T, normed_two, preferred_element_type=jnp.float32)
    hidden = (jax.nn.silu(gate) * upward).astype(jnp.bfloat16)
    ffn_out = block_sum(w_down, hidden, N_TP)
    final = after_mix + ffn_out
    return (final * rms_factor(final) * gain_out[:, None]).astype(jnp.bfloat16)
```

```python
import functools

import jax
import jax.numpy as jnp
from jax import lax
from jax.experimental import pallas as pl
from jax.experimental.pallas import tpu as pltpu
from jax.sharding import PartitionSpec as P

POOL_GROUP = 256
SEQ_LEN = 256
EPS = 1e-06
LANES = 128
MESH = pl.DeviceIdType.MESH
BF = jnp.bfloat16
F32 = jnp.float32


def dot_first(weights, acts):
    return lax.dot_general(weights, acts, (((0,), (0,)), ((), ())), preferred_element_type=F32)


def column(row, width):
    square = jnp.transpose(jnp.broadcast_to(row, (LANES, LANES)))
    return jnp.concatenate([square] * (width // LANES), axis=1)


def body(
    nr, nf, nt,
    act, w_in, w_out, w_gate, w_up, w_down, scale, g_mix, g_ffn, g_out, out,
    b_in, b_out, b_gate, b_up, b_down,
    h, x1, part0, part1, u_acc, pooled, gate_acc, up_acc, hidden, own_x, squares,
    buf_a, buf_b,
    own_sem, zsend, zrecv, ysend, yrecv,
    a_send, a_recv, b_send, b_recv, c_send, c_recv, d_send, d_recv, s_send, s_recv,
):
    r, f, t = lax.axis_index("rep"), lax.axis_index("fs"), lax.axis_index("tp")
    features, tokens = act.shape
    shards = (w_in, w_out, w_gate, w_up, w_down)
    full = (b_in, b_out, b_gate, b_up, b_down)
    rows = w_in.shape[0]
    piece = rows // nr
    share = features // nt
    channels = w_in.shape[1]
    ff = w_gate.shape[1]
    nh = nt // 2
    chip, parity = t // 2, lax.rem(t, 2)
    partner = t + 1 - 2 * parity

    cut = -(-ff // (2 * LANES)) * LANES
    items = [(0, 0, channels), (1, 0, channels)]
    for m in (2, 3, 4):
        items += [(m, 0, cut), (m, cut, ff - cut)]

    own = [pltpu.make_async_copy(shards[m], full[m].at[f], own_sem.at[m]) for m in range(5)]
    for copy in own:
        copy.start()

    barrier = pltpu.get_barrier_semaphore()
    for step in (1, nf - 1):
        pl.semaphore_signal(barrier, inc=1, device_id=(r, lax.rem(f + step, nf), t), device_id_type=MESH)
    for o in range(1, nr):
        pl.semaphore_signal(barrier, inc=1, device_id=(lax.rem(r + o, nr), f, t), device_id_type=MESH)
    for i in range(1, nt):
        pl.semaphore_signal(barrier, inc=1, device_id=(r, f, lax.rem(t + i, nt)), device_id_type=MESH)
    pl.semaphore_wait(barrier, 2 + (nr - 1) + (nt - 1))

    def part_of(m, blk, of):
        matrix, start, size = items[m]
        at = pl.ds(pl.multiple_of(of * piece, piece), piece)
        return full[matrix].at[blk, at, pl.ds(start, size)]

    def z_copy(m, blk, way, d):
        ref = part_of(m, blk, r)
        return pltpu.make_async_remote_copy(
            src_ref=ref, dst_ref=ref,
            send_sem=zsend.at[m, way, lax.rem(d, 2)], recv_sem=zrecv.at[m, blk],
            device_id=(r, f + 1 - 2 * way, t), device_id_type=MESH,
        )

    def y_copy(m, blk, way, d, o):
        ref = part_of(m, blk, r)
        return pltpu.make_async_remote_copy(
            src_ref=ref, dst_ref=ref,
            send_sem=ysend.at[m, way, lax.rem(d, 2), o - 1], recv_sem=yrecv.at[m, blk, o - 1],
            device_id=(lax.rem(r + o, nr), f, t), device_id_type=MESH,
        )

    def y_arrival(m, blk, o):
        source = lax.rem(r - o + nr, nr)
        ref = part_of(m, blk, source)
        return pltpu.make_async_remote_copy(
            src_ref=ref, dst_ref=ref,
            send_sem=ysend.at[m, 0, 0, o - 1], recv_sem=yrecv.at[m, blk, o - 1],
            device_id=(lax.rem(r + o, nr), f, t), device_id_type=MESH,
        )

    can_send = (f + 1 < nf, f >= 1)
    hops = (f, nf - 1 - f)

    def send_own(m):
        if items[m][1] == 0:
            own[items[m][0]].wait()
        for way in (0, 1):
            @pl.when(can_send[way])
            def _():
                z_copy(m, f, way, 0).start()

    def arrival(m, way, d):
        blk = f - d if way == 0 else f + d

        @pl.when(d <= hops[way])
        def _():
            z_copy(m, blk, way, d).wait_recv()

            @pl.when(can_send[way])
            def _():
                @pl.when(d >= 2)
                def _():
                    z_copy(m, blk, way, d).wait_send()

                z_copy(m, blk, way, d).start()

            for o in range(1, nr):
                @pl.when(d >= 3)
                def _():
                    y_copy(m, blk, way, d, o).wait_send()

                y_copy(m, blk, way, d, o).start()

    def gather(m, low, high):
        if low >= high:
            return

        def rounds(d, carry):
            arrival(m, 0, d)
            arrival(m, 1, d)
            return carry

        if low == 1:
            rounds(jnp.int32(1), 0)
            if m + 1 < len(items):
                send_own(m + 1)
            low = 2
        lax.fori_loop(low, high, rounds, 0)

    def finish(m):
        def one(blk, carry):
            @pl.when(blk != f)
            def _():
                for o in range(1, nr):
                    y_arrival(m, blk, o).wait_recv()
            return carry

        lax.fori_loop(0, nf, one, 0)

    def drain(m):
        for way in (0, 1):
            for back in (0, 1):
                last = hops[way] - back

                @pl.when(jnp.logical_and(can_send[way], last >= 0))
                def _():
                    z_copy(m, f, way, last).wait_send()

                @pl.when(last >= 1)
                def _():
                    for o in range(1, nr):
                        y_copy(m, f, way, last, o).wait_send()

    def share_of(ref, j):
        return ref.at[pl.ds(pl.multiple_of(j * share, share), share), :]

    def normalize(load, gain, store, count):
        def square(i, total):
            v = load(i)
            return total + jnp.sum(v * v, axis=0, keepdims=True)

        total = lax.fori_loop(0, count, square, jnp.zeros((1, tokens), F32))
        factor = lax.rsqrt(total / features + EPS)

        def scaled(i, carry):
            store(i, load(i) * factor * column(gain[pl.ds(i, 1), :], tokens))
            return carry

        lax.fori_loop(0, count, scaled, 0)

    def chunk(ref, i):
        return ref[pl.ds(pl.multiple_of(i * LANES, LANES), LANES), :].astype(F32)

    def put(ref):
        def store(i, v):
            ref[pl.ds(pl.multiple_of(i * LANES, LANES), LANES), :] = v.astype(ref.dtype)
        return store

    def a_copy(k, part, c):
        return pltpu.make_async_remote_copy(
            src_ref=share_of(part, 2 * c + 1 - parity), dst_ref=buf_a.at[k, c],
            send_sem=a_send.at[k, c], recv_sem=a_recv.at[k, c],
            device_id=(r, f, partner), device_id_type=MESH,
        )

    def b_copy(k, part, i):
        target = 2 * lax.rem(chip + i, nh) + parity
        return pltpu.make_async_remote_copy(
            src_ref=share_of(part, target), dst_ref=buf_b.at[k, i],
            send_sem=b_send.at[k, i], recv_sem=b_recv.at[k, i],
            device_id=(r, f, target), device_id_type=MESH,
        )

    def start_pair(k, part):
        for i in range(nh):
            a_copy(k, part, i).start()

    def start_chips(k, part):
        for i in range(1, nh):
            c = lax.rem(chip + i, nh)
            target = 2 * c + parity
            a_copy(k, part, c).wait()

            def add(n, carry):
                at = pl.ds(pl.multiple_of(target * share + n * LANES, LANES), LANES)
                mine = part[at, :].astype(F32)
                theirs = buf_a[k, c, pl.ds(pl.multiple_of(n * LANES, LANES), LANES), :].astype(F32)
                part[at, :] = (mine + theirs).astype(BF)
                return carry

            lax.fori_loop(0, share // LANES, add, 0)
            b_copy(k, part, i).start()

    def finish_chips(k, part, base, store):
        a_copy(k, part, chip).wait()
        for i in range(1, nh):
            b_copy(k, part, i).wait()

        def add(n, carry):
            here = pl.ds(pl.multiple_of(n * LANES, LANES), LANES)
            at = pl.ds(pl.multiple_of(t * share + n * LANES, LANES), LANES)
            total = part[at, :].astype(F32) + buf_a[k, chip, here, :].astype(F32)
            for i in range(1, nh):
                total = total + buf_b[k, i, here, :].astype(F32)
            store(n, base[at, :].astype(F32) + total)
            return carry

        lax.fori_loop(0, share // LANES, add, 0)

    def c_copy(i):
        ref = share_of(x1, t)
        return pltpu.make_async_remote_copy(
            src_ref=ref, dst_ref=ref, send_sem=c_send.at[i], recv_sem=c_recv.at[i],
            device_id=(r, f, 2 * lax.rem(chip + i, nh) + parity), device_id_type=MESH,
        )

    def d_copy(i):
        ref = share_of(x1, 2 * lax.rem(chip - i + nh, nh) + parity)
        return pltpu.make_async_remote_copy(
            src_ref=ref, dst_ref=ref, send_sem=d_send.at[i], recv_sem=d_recv.at[i],
            device_id=(r, f, partner), device_id_type=MESH,
        )

    def s_copy(i):
        return pltpu.make_async_remote_copy(
            src_ref=squares.at[0], dst_ref=squares.at[i], send_sem=s_send.at[i], recv_sem=s_recv.at[i],
            device_id=(r, f, lax.rem(t + i, nt)), device_id_type=MESH,
        )

    send_own(0)
    normalize(functools.partial(chunk, act), g_mix, put(h), features // LANES)

    gather(0, 1, nf)
    gather(1, 1, nf)
    finish(0)
    u_acc[...] = jnp.zeros_like(u_acc)

    def mix_in(b, carry):
        at = pl.ds(pl.multiple_of(b * rows, rows), rows)
        u_acc[...] += dot_first(b_in[b], h[at, :])
        return carry

    lax.fori_loop(0, nf, mix_in, 0)
    for i in range(channels // LANES):
        first = t * channels + i * LANES
        window = jnp.int32(2) << (first // POOL_GROUP)
        behind = window // 2
        onward = window - behind
        source = lax.broadcasted_iota(jnp.int32, (SEQ_LEN, SEQ_LEN), 0)
        place = lax.broadcasted_iota(jnp.int32, (SEQ_LEN, SEQ_LEN), 1)
        inside = jnp.logical_and(source >= place - behind, source < place + onward)
        band = jnp.where(inside, 1.0, 0.0).astype(BF)
        spot = lax.broadcasted_iota(jnp.int32, (1, SEQ_LEN), 1)
        count = (jnp.minimum(spot + onward, SEQ_LEN) - jnp.maximum(spot - behind, 0)).astype(F32)
        gain = column(scale[pl.ds(first // LANES, 1), :], SEQ_LEN)
        for s in range(tokens // SEQ_LEN):
            at = (pl.ds(i * LANES, LANES), pl.ds(s * SEQ_LEN, SEQ_LEN))
            u = u_acc[at].astype(BF)
            mean = jnp.dot(u, band, preferred_element_type=F32) / count
            pooled[at] = ((mean - u.astype(F32)) * gain).astype(BF)

    gather(2, 1, nf)
    finish(1)

    def mix_out(b, carry):
        at = pl.ds(pl.multiple_of(b * rows, rows), rows)
        part0[at, :] = jnp.dot(b_out[b], pooled[...], preferred_element_type=F32).astype(BF)
        return carry

    lax.fori_loop(0, nf, mix_out, 0)
    start_pair(0, part0)
    gather(3, 1, nf)
    start_chips(0, part0)
    gather(4, 1, nf)

    def keep_x1(n, v):
        at = pl.ds(pl.multiple_of(t * share + n * LANES, LANES), LANES)
        x1[at, :] = v.astype(BF)

    finish_chips(0, part0, act, keep_x1)
    for i in range(1, nh):
        c_copy(i).start()
    d_copy(0).start()
    gather(5, 1, nf)
    for i in range(1, nh):
        c_copy(i).wait()
        d_copy(i).start()
    gather(6, 1, nf)
    for i in range(nh):
        d_copy(i).wait()
    normalize(functools.partial(chunk, x1), g_ffn, put(h), features // LANES)
    finish(2)
    finish(3)
    gate_acc[...] = jnp.zeros_like(gate_acc)
    up_acc[...] = jnp.zeros_like(up_acc)

    def project(source, acc):
        def one(b, carry):
            at = pl.ds(pl.multiple_of(b * rows, rows), rows)
            acc[...] += dot_first(source[b], h[at, :])
            return carry

        lax.fori_loop(0, nf, one, 0)

    gather(7, 1, nf)
    project(b_gate, gate_acc)
    finish(4)
    finish(5)
    project(b_up, up_acc)
    step = 32

    def activate(n, carry):
        at = pl.ds(pl.multiple_of(n * step, step), step)
        v = gate_acc[at, :]
        hidden[at, :] = (v / (1.0 + jnp.exp(-v)) * up_acc[at, :]).astype(BF)
        return carry

    lax.fori_loop(0, ff // step, activate, 0)
    finish(6)
    finish(7)

    def mlp_out(b, carry):
        at = pl.ds(pl.multiple_of(b * rows, rows), rows)
        part1[at, :] = jnp.dot(b_down[b], hidden[...], preferred_element_type=F32).astype(BF)
        return carry

    if share % rows == 0:
        blocks = share // rows

        def pair_out(c):
            theirs, ours = 2 * c + 1 - parity, 2 * c + parity
            lax.fori_loop(theirs * blocks, (theirs + 1) * blocks, mlp_out, 0)
            a_copy(1, part1, c).start()
            lax.fori_loop(ours * blocks, (ours + 1) * blocks, mlp_out, 0)

        for i in range(1, nh):
            pair_out(lax.rem(chip + i, nh))
        start_chips(1, part1)
        pair_out(chip)
    else:
        lax.fori_loop(0, nf, mlp_out, 0)
        start_pair(1, part1)
        start_chips(1, part1)
    for m in range(len(items)):
        drain(m)
    finish_chips(1, part1, x1, put(own_x))

    def square(i, total):
        v = chunk(own_x, i)
        return total + jnp.sum(v * v, axis=0, keepdims=True)

    mine = lax.fori_loop(0, share // LANES, square, jnp.zeros((1, tokens), F32))
    squares[0] = jnp.broadcast_to(mine, squares.shape[1:])
    for i in range(1, nt):
        s_copy(i).start()
    for i in range(1, nt):
        s_copy(i).wait()
    total = squares[0, pl.ds(0, 1), :]
    for i in range(1, nt):
        total = total + squares[i, pl.ds(0, 1), :]
    factor = lax.rsqrt(total / features + EPS)

    def closing(i, carry):
        gain = column(g_out[pl.ds(t * (share // LANES) + i, 1), :], tokens)
        put(out)(i, chunk(own_x, i) * factor * gain)
        return carry

    lax.fori_loop(0, share // LANES, closing, 0)


def staged(
    nr, nf, nt,
    act, w_in, w_out, w_gate, w_up, w_down, scale, g_mix, g_ffn, g_out, out,
    b_in, b_out, b_gate, b_up, b_down,
    x0, h, x1, part, pooled, gate_acc, up_acc, hidden, own_x, squares,
    buf_a, buf_b, back, home,
    own_sem, act_sem, in_send, out_send, zrecv, wsend, wrecv, ysend, yrecv, v_send, v_recv,
    a_send, a_recv, b_send, b_recv, c_send, c_recv, d_send, d_recv,
    e_send, e_recv, g_send, g_recv, s_send, s_recv,
):
    r, f, t = lax.axis_index("rep"), lax.axis_index("fs"), lax.axis_index("tp")
    features, tokens = act.shape
    shards = (w_in, w_out, w_gate, w_up, w_down)
    full = (b_in, b_out, b_gate, b_up, b_down)
    rows, channels = w_in.shape
    ff = w_gate.shape[0]
    share = features // nt
    nh = nt // 2
    nq = share // LANES
    chip, parity = t // 2, lax.rem(t, 2)
    partner = t + 1 - 2 * parity
    other_rep = lax.rem(r + 1, nr)
    cuts = 2
    slab = share // cuts
    items = [(0, 0), (0, 1), (1, 0), (1, 1), (2, 0), (3, 0), (2, 1), (3, 1), (4, 0), (4, 1)]
    early = 4
    extra = 7
    last = len(items)
    left = f < nf // 2
    inner = jnp.logical_and(f >= 1, f < nf - 1)
    outer = jnp.logical_not(inner)
    mate = jnp.where(left, 1 - f, 2 * nf - 3 - f)
    inward = jnp.where(left, f + 1, f - 1)
    over = jnp.where(inner, nf - 1 - f, nf - 1 - mate)
    far = jnp.where(inner, nf - 1 - mate, nf - 1 - f)
    blocks = (mate, over, far)

    own = [pltpu.make_async_copy(shards[m], full[m].at[f], own_sem.at[m]) for m in range(5)]
    quarter = features // 4
    stream = [
        pltpu.make_async_copy(act.at[pl.ds(i * quarter, quarter)], x0.at[pl.ds(i * quarter, quarter)], act_sem.at[i])
        for i in range(4)
    ]
    own[0].start()
    own[1].start()
    for copy in stream:
        copy.start()
    for copy in own[2:]:
        copy.start()

    barrier = pltpu.get_barrier_semaphore()
    for step in (1, nf - 1):
        pl.semaphore_signal(barrier, inc=1, device_id=(r, lax.rem(f + step, nf), t), device_id_type=MESH)
    pl.semaphore_signal(barrier, inc=1, device_id=(other_rep, f, t), device_id_type=MESH)
    for i in range(1, nt):
        pl.semaphore_signal(barrier, inc=1, device_id=(r, f, lax.rem(t + i, nt)), device_id_type=MESH)
    pl.semaphore_wait(barrier, 3 + (nt - 1))

    def line(start, size=LANES):
        return pl.ds(pl.multiple_of(start, size), size)

    def part_of(m, blk, of):
        matrix, s = items[m]
        if matrix < 2:
            size = rows // cuts // nr
            return full[matrix].at[blk, line((s * nr + of) * size, size), :]
        if matrix < 4:
            size = ff // cuts // nr
            return full[matrix].at[blk, line((s * nr + of) * size, size), :]
        size = rows // cuts // nr
        return full[matrix].at[blk, :, line((s * nr + of) * size, size)]

    def remote(ref, dst, send, recv, device):
        return pltpu.make_async_remote_copy(
            src_ref=ref, dst_ref=dst, send_sem=send, recv_sem=recv, device_id=device, device_id_type=MESH
        )

    def in_copy(m, blk, d):
        ref = part_of(m, blk, r)
        return remote(ref, ref, in_send.at[m, d], zrecv.at[m, blk], (r, inward, t))

    def out_copy(m, blk, d):
        ref = part_of(m, blk, r)
        return remote(ref, ref, out_send.at[m, d], zrecv.at[m, blk], (r, mate, t))

    def w_copy(m, blk):
        ref = part_of(m, blk, other_rep)
        return remote(ref, ref, wsend.at[m], wrecv.at[m], (r, mate, t))

    def v_copy(blk):
        ref = part_of(extra, blk, other_rep)
        return remote(ref, ref, v_send.at[0], v_recv.at[0], (r, inward, t))

    def y_copy(m, blk, of):
        ref = part_of(m, blk, of)
        return remote(ref, ref, ysend.at[m, blk], yrecv.at[m, blk], (other_rep, f, t))

    def own_ready(m):
        if items[m][1] == 0:
            own[items[m][0]].wait()

    def send_mixer(m):
        own_ready(m)
        in_copy(m, f, 0).start()

        @pl.when(inner)
        def _():
            out_copy(m, f, 0).start()

    def hop(m, j):
        blk = blocks[j]
        in_copy(m, blk, 0).wait_recv()
        if j == 0:
            in_copy(m, blk, 1).start()
        else:
            out_copy(m, blk, j).start()

    def side(m, j):
        y_copy(m, blocks[j], r).start()

    def relay(m, j):
        hop(m, j)
        side(m, j)

    def collect(m, j):
        in_copy(m, blocks[j], 0).wait_recv()
        y_copy(m, blocks[j], r).start()

    def y_arrival(m, blk):
        y_copy(m, blk, other_rep).wait_recv()

    def finish(m):
        for blk in blocks:
            y_arrival(m, blk)

    def send_inner(m):
        in_copy(m, f, 0).start()

    def send_outer(m):
        in_copy(m, f, 0).start()
        w_copy(m, f).start()

    def pass_on(m):
        if m < last:
            in_copy(m, mate, 0).wait_recv()
            in_copy(m, mate, 1).start()

    def cross(m, *some):
        for blk in some:
            in_copy(m, blk, 0).wait_recv()
            if m != extra or blk is far:
                y_copy(m, blk, r).start()

    def settle(m):
        w_copy(m, mate).wait_recv()
        if m == extra:
            v_copy(over).wait_recv()
        else:
            y_arrival(m, over)
        y_arrival(m, far)

    def spot(target, q, size=LANES):
        return line(target * share + q * size, size)

    def normalize(load, gain, store, count):
        def square(i, total):
            v = load(i)
            return total + jnp.sum(v * v, axis=0, keepdims=True)

        total = lax.fori_loop(0, count, square, jnp.zeros((1, tokens), F32))
        factor = lax.rsqrt(total / features + EPS)

        def scaled(i, carry):
            store(i, load(i) * factor * column(gain[pl.ds(i, 1), :], tokens))
            return carry

        lax.fori_loop(0, count, scaled, 0)

    def chunk(ref, i):
        return ref[line(i * LANES), :].astype(F32)

    def put(ref):
        def store(i, v):
            ref[line(i * LANES), :] = v.astype(ref.dtype)
        return store

    def a_copy(k, target, q, size):
        return remote(
            part.at[k, spot(target, q, size)], buf_a.at[k, target // 2, line(q * size, size)],
            a_send.at[k, target // 2, q], a_recv.at[k, target // 2, q], (r, f, partner),
        )

    def b_copy(k, i, q, size):
        target = 2 * lax.rem(chip + i, nh) + parity
        return remote(
            part.at[k, spot(target, q, size)], buf_b.at[k, i, line(q * size, size)],
            b_send.at[k, i, q], b_recv.at[k, i, q], (r, f, target),
        )

    def c_copy(k, i, q):
        ref = x1.at[k, spot(t, q)]
        device = (r, f, 2 * lax.rem(chip + i, nh) + parity)
        return remote(ref, ref, c_send.at[k, i, q], c_recv.at[k, i, q], device)

    def d_copy(k, i, q):
        ref = x1.at[k, spot(2 * lax.rem(chip - i + nh, nh) + parity, q)]
        return remote(ref, ref, d_send.at[k, i, q], d_recv.at[k, i, q], (r, f, partner))

    def e_copy(q):
        return remote(x1.at[0, spot(t, q)], x1.at[1, spot(t, q)], e_send.at[q], e_recv.at[q], (r, mate, t))

    def g_copy(q):
        return remote(back.at[line(q * LANES)], home.at[line(q * LANES)], g_send.at[q], g_recv.at[q], (r, mate, t))

    def s_copy(i):
        return remote(squares.at[0], squares.at[i], s_send.at[i], s_recv.at[i], (r, f, lax.rem(t + i, nt)))

    def add_pair(k, target, q, size):
        for n in range(size // LANES):
            here = line(q * size + n * LANES)
            at = line(target * share + q * size + n * LANES)
            mine, theirs = part[k, at, :].astype(F32), buf_a[k, target // 2, here, :].astype(F32)
            part[k, at, :] = (mine + theirs).astype(BF)

    def total_of(k, q):
        here = line(q * LANES)
        total = part[k, spot(t, q), :].astype(F32) + buf_a[k, chip, here, :].astype(F32)
        for i in range(1, nh):
            total = total + buf_b[k, i, here, :].astype(F32)
        return total

    send_mixer(0)
    send_mixer(1)
    for m in (2, 4, 5, 8):
        own_ready(m)

    @pl.when(outer)
    def _():
        for m in (2, 3):
            in_copy(m, f, 0).start()
        for m in (4, 5, 6):
            send_outer(m)
        in_copy(7, f, 0).start()

    @pl.when(inner)
    def _():
        in_copy(2, f, 0).start()

    for copy in stream:
        copy.wait()
    normalize(functools.partial(chunk, x0), g_mix, put(h.at[0]), features // LANES)

    @pl.when(inner)
    def _():
        relay(0, 0)
        relay(0, 1)
        relay(1, 0)
        relay(1, 1)
        in_copy(3, f, 0).start()
        hop(2, 0)
        hop(3, 0)
        send_inner(4)
        for m in (2, 3):
            out_copy(m, f, 0).start()
        relay(0, 2)
        relay(1, 2)
        side(2, 0)
        side(3, 0)
        relay(2, 1)
        relay(3, 1)
        pass_on(4)
        send_inner(5)

    @pl.when(outer)
    def _():
        for j in range(3):
            collect(0, j)
            collect(1, j)

    finish(0)
    finish(1)

    u_mix = dot_first(b_in[0], h[0, pl.ds(0, rows), :])
    for b in range(1, nf):
        u_mix += dot_first(b_in[b], h[0, pl.ds(b * rows, rows), :])
    gate_acc[pl.ds(0, channels), :] = u_mix
    for i in range(channels // LANES):
        first = t * channels + i * LANES
        window = jnp.int32(2) << (first // POOL_GROUP)
        behind = window // 2
        onward = window - behind
        source = lax.broadcasted_iota(jnp.int32, (SEQ_LEN, SEQ_LEN), 0)
        place = lax.broadcasted_iota(jnp.int32, (SEQ_LEN, SEQ_LEN), 1)
        inside = jnp.logical_and(source >= place - behind, source < place + onward)
        band = jnp.where(inside, 1.0, 0.0).astype(BF)
        seat = lax.broadcasted_iota(jnp.int32, (1, SEQ_LEN), 1)
        count = (jnp.minimum(seat + onward, SEQ_LEN) - jnp.maximum(seat - behind, 0)).astype(F32)
        gain = column(scale[pl.ds(first // LANES, 1), :], SEQ_LEN)
        for s in range(tokens // SEQ_LEN):
            at = (pl.ds(i * LANES, LANES), pl.ds(s * SEQ_LEN, SEQ_LEN))
            u = gate_acc[at].astype(BF)
            mean = jnp.dot(u, band, preferred_element_type=F32) / count
            pooled[at] = ((mean - u.astype(F32)) * gain).astype(BF)

    mixed = True

    @pl.when(inner)
    def _():
        relay(2, 2)
        relay(3, 2)
        cross(4, over)
        pass_on(5)
        send_inner(6)
        cross(4, far)

    @pl.when(outer)
    def _():
        for j in range(3):
            collect(2, j)
            collect(3, j)

    finish(2)
    finish(3)

    def mix_out(target):
        part[0, line(target * share, share), :] = jnp.dot(
            b_out[target], pooled[...], preferred_element_type=F32
        ).astype(BF)

    for i in range(1, nh + 1):
        c = lax.rem(chip + i, nh)
        mix_out(2 * c + 1 - parity)
        a_copy(0, 2 * c + 1 - parity, 0, share).start()
        mix_out(2 * c + parity)
    for i in range(1, nh):
        target = 2 * lax.rem(chip + i, nh) + parity
        a_copy(0, target, 0, share).wait_recv()
        for q in range(nq):
            add_pair(0, target, q, LANES)
            b_copy(0, i, q, LANES).start()
    a_copy(0, t, 0, share).wait_recv()

    @pl.when(inner)
    def _():
        cross(5, over)

    for q in range(nq):
        for i in range(1, nh):
            b_copy(0, i, q, LANES).wait_recv()
        x1[0, spot(t, q), :] = (x0[spot(t, q), :].astype(F32) + total_of(0, q)).astype(BF)

        @pl.when(inner)
        def _():
            for i in range(1, nh):
                c_copy(0, i, q).start()
            d_copy(0, 0, q).start()
            if q == 0:
                pass_on(6)
                send_inner(7)
                cross(5, far)
            if q == 1:
                cross(6, over)
            if q == 2:
                pass_on(7)
                send_inner(8)
                v_copy(f).start()

        @pl.when(outer)
        def _():
            e_copy(q).start()
            if q == 0:
                w_copy(7, f).start()
            if q == 1:
                in_copy(8, f, 0).start()
            if q == 3:
                in_copy(9, f, 0).start()

    cut = ff // cuts
    step = 32
    wide = 2 * LANES

    def project(k, s):
        at = pl.ds(s * cut, cut)
        for source, acc in ((b_gate, gate_acc), (b_up, up_acc)):
            def tokens_at(n, carry):
                here = line(n * wide, wide)
                total = jnp.dot(source[0, at, :], h[k, pl.ds(0, rows), here], preferred_element_type=F32)
                for b in range(1, nf):
                    total += jnp.dot(source[b, at, :], h[k, pl.ds(b * rows, rows), here], preferred_element_type=F32)
                acc[at, here] = total
                return carry

            lax.fori_loop(0, tokens // wide, tokens_at, 0)

        def activate(n, carry):
            here = line(s * cut + n * step, step)
            v = gate_acc[here, :]
            hidden[k, here, :] = (v / (1.0 + jnp.exp(-v)) * up_acc[here, :]).astype(BF)
            return carry

        lax.fori_loop(0, cut // step, activate, 0)

    def mlp_out(k, target, s):
        at = spot(target, s, slab)
        part[1 + k, at, :] = dot_first(b_down[target, :, line(s * slab, slab)], hidden[k]).astype(BF)

        @pl.when(lax.rem(target, 2) != parity)
        def _():
            a_copy(1 + k, target, s, slab).start()

    def pair_up(k, target, s):
        @pl.when(lax.rem(target, 2) == parity)
        def _():
            a_copy(1 + k, target, s, slab).wait_recv()
            for i in range(1, nh):
                @pl.when(target // 2 == lax.rem(chip + i, nh))
                def _():
                    add_pair(1 + k, target, s, slab)
                    b_copy(1 + k, i, s, slab).start()

    plans = (
        [(1, 2, 0), (1, 3, 0), (1, 2, 1), (1, 3, 1), (0, 3, 1), (1, 0, 0), (1, 0, 1), (1, 1, 0), (1, 1, 1),
         (0, 0, 0), (0, 0, 1), (0, 1, 0), (0, 1, 1)],
        [(1, 0, 0), (1, 0, 1), (1, 1, 0), (1, 1, 1), (0, 1, 1), (1, 2, 0), (1, 3, 0), (1, 2, 1), (1, 3, 1),
         (0, 2, 0), (0, 3, 0), (0, 2, 1), (0, 3, 1)],
    )
    near = chip == f // 2

    def planned(n):
        k, s, target = jnp.int32(0), jnp.int32(0), f
        for plan, taken in zip(plans, (near, jnp.logical_not(near))):
            for at, (kk, code, ss) in enumerate(plan):
                here = jnp.logical_and(n == at, taken)
                k = jnp.where(here, kk, k)
                s = jnp.where(here, ss, s)
                target = jnp.where(here, (f, mate, over, far)[code], target)
        return k, target, s

    def give_back(s):
        for i in range(1, nh):
            b_copy(2, i, s, slab).wait_recv()
        for n in range(slab // LANES):
            q = s * (slab // LANES) + n
            back[pl.ds(q * LANES, LANES), :] = total_of(2, q).astype(BF)
            g_copy(q).start()

    def spread(q):
        e_copy(q).wait_recv()
        for i in range(1, nh):
            c_copy(1, i, q).start()
        d_copy(1, 0, q).start()

    def hand_over(k, q):
        for i in range(1, nh):
            c_copy(k, i, q).wait_recv()
            d_copy(k, i, q).start()

    def second_norm(k):
        for q in range(nq):
            for i in range(nh):
                d_copy(k, i, q).wait_recv()
        normalize(functools.partial(chunk, x1.at[k]), g_ffn, put(h.at[k]), features // LANES)

    @pl.when(inner)
    def _():
        cross(6, far)
        hand_over(0, 0)
        cross(7, over)
        hand_over(0, 1)
        spread(0)
        cross(7, far)
        hand_over(0, 2)
        spread(1)
        pass_on(8)
        send_inner(9)
        cross(8, over)
        hand_over(0, 3)
        spread(2)
        second_norm(0)
        cross(8, far)
        spread(3)
        settle(4)
        settle(5)
        project(0, 0)
        pass_on(9)
        hand_over(1, 0)
        hand_over(1, 1)
        settle(6)
        settle(7)
        project(0, 1)
        cross(9, over)

        @pl.when(near)
        def _():
            y_arrival(8, over)
            mlp_out(0, over, 0)

        @pl.when(jnp.logical_not(near))
        def _():
            mlp_out(0, f, 0)
            mlp_out(0, f, 1)
            pair_up(0, f, 0)

        hand_over(1, 2)
        hand_over(1, 3)
        pair_up(0, jnp.where(near, over, f), jnp.where(near, 0, 1))
        second_norm(1)
        cross(9, far)

        @pl.when(near)
        def _():
            y_arrival(8, far)

        @pl.when(jnp.logical_not(near))
        def _():
            w_copy(8, mate).wait_recv()

        ahead = jnp.where(near, far, mate)
        mlp_out(0, ahead, 0)
        project(1, 0)
        pair_up(0, ahead, 0)

        @pl.when(near)
        def _():
            y_arrival(9, over)
            mlp_out(0, over, 1)

        project(1, 1)

        @pl.when(near)
        def _():
            pair_up(0, over, 1)


        def ffn(n, carry):
            near_waits = (
                (3, lambda: y_arrival(9, far)),
                (7, lambda: w_copy(8, mate).wait_recv()),
                (8, lambda: w_copy(9, mate).wait_recv()),
            )
            away_waits = (
                (3, lambda: w_copy(9, mate).wait_recv()),
                (5, lambda: y_arrival(8, over)),
                (6, lambda: y_arrival(8, far)),
                (7, lambda: y_arrival(9, over)),
                (8, lambda: y_arrival(9, far)),
            )
            for waits, taken in ((near_waits, near), (away_waits, jnp.logical_not(near))):
                for at, wait in waits:
                    @pl.when(jnp.logical_and(n == at, taken))
                    def _():
                        wait()

            @pl.when(n == 10)
            def _():
                give_back(0)

            mlp_out(*planned(n))

            @pl.when(n >= 1)
            def _():
                pair_up(*planned(n - 1))
            return carry

        lax.fori_loop(0, len(plans[0]), ffn, 0)
        pair_up(*planned(len(plans[0]) - 1))
        give_back(1)
        for q in range(nq):
            for i in range(1, nh):
                if q % (slab // LANES) == 0:
                    b_copy(1, i, q // (slab // LANES), slab).wait_recv()
            own_x[pl.ds(q * LANES, LANES), :] = x1[0, spot(t, q), :].astype(F32) + total_of(1, q)

    @pl.when(outer)
    def _():
        for m in (8, 9):
            w_copy(m, f).start()
        for q in range(nq):
            g_copy(q).wait_recv()
            at = pl.ds(q * LANES, LANES)
            own_x[at, :] = x1[0, spot(t, q), :].astype(F32) + home[at, :].astype(F32)

    total = jnp.zeros((1, tokens), F32)
    for q in range(nq):
        v = own_x[pl.ds(q * LANES, LANES), :]
        total += jnp.sum(v * v, axis=0, keepdims=True)
    squares[0] = jnp.broadcast_to(total, squares.shape[1:])
    for i in range(1, nt):
        s_copy(i).start()

    for i in range(1, nt):
        s_copy(i).wait()
    for i in range(1, nt):
        total = total + squares[i, pl.ds(0, 1), :]
    factor = lax.rsqrt(total / features + EPS)

    def closing(q):
        gain = column(g_out[pl.ds(t * nq + q, 1), :], tokens)
        out[pl.ds(q * LANES, LANES), :] = (own_x[pl.ds(q * LANES, LANES), :] * factor * gain).astype(BF)

    for q in range(nq):
        closing(q)

    for m in range(last):
        in_copy(m, f, 0).wait_send()
    for m in range(early):
        for blk in blocks:
            y_copy(m, blk, r).wait_send()
    for i in range(1, nh + 1):
        c = lax.rem(chip + i, nh)
        a_copy(0, 2 * c + 1 - parity, 0, share).wait_send()
    for i in range(1, nh):
        for q in range(nq):
            b_copy(0, i, q, LANES).wait_send()

    @pl.when(inner)
    def _():
        for m in range(last):
            in_copy(m, mate, 1).wait_send()
        for m in range(early):
            for j, blk in enumerate((f, over, far)):
                out_copy(m, blk, j).wait_send()
        for m in range(early, last):
            if m != extra:
                y_copy(m, over, r).wait_send()
            y_copy(m, far, r).wait_send()
        v_copy(f).wait_send()
        for k in (0, 1):
            for i in range(nh):
                for s in range(cuts):
                    a_copy(1 + k, 2 * i + 1 - parity, s, slab).wait_send()
                    if i:
                        b_copy(1 + k, i, s, slab).wait_send()
                for q in range(nq):
                    d_copy(k, i, q).wait_send()
                    if i:
                        c_copy(k, i, q).wait_send()
        for q in range(nq):
            g_copy(q).wait_send()

    @pl.when(outer)
    def _():
        for m in range(early, last):
            w_copy(m, f).wait_send()
        for q in range(nq):
            e_copy(q).wait_send()


def solution(mesh):
    nr, nf, nt = mesh.shape["rep"], mesh.shape["fs"], mesh.shape["tp"]

    def staged_call(act, w_in, w_out, w_gate, w_up, w_down, scale, g_mix, g_ffn, g_out):
        features, tokens = act.shape
        rows, channels = w_in.shape
        ff = w_gate.shape[1]
        share = features // nt
        nh = nt // 2
        nq = share // LANES
        anywhere = pl.BlockSpec(memory_space=pl.ANY)
        vmem = pl.BlockSpec(memory_space=pltpu.VMEM)
        dma = pltpu.SemaphoreType.DMA
        scratch = [
            pltpu.VMEM((nf, rows, channels), BF),
            pltpu.VMEM((nf, rows, channels), BF),
            pltpu.VMEM((nf, ff, rows), BF),
            pltpu.VMEM((nf, ff, rows), BF),
            pltpu.VMEM((nf, ff, rows), BF),
            pltpu.VMEM((features, tokens), BF),
            pltpu.VMEM((2, features, tokens), BF),
            pltpu.VMEM((2, features, tokens), BF),
            pltpu.VMEM((3, features, tokens), BF),
            pltpu.VMEM((channels, tokens), BF),
            pltpu.VMEM((ff, tokens), F32),
            pltpu.VMEM((ff, tokens), F32),
            pltpu.VMEM((2, ff, tokens), BF),
            pltpu.VMEM((share, tokens), F32),
            pltpu.VMEM((nt, 8, tokens), F32),
            pltpu.VMEM((3, nh, share, tokens), BF),
            pltpu.VMEM((3, nh, share, tokens), BF),
            pltpu.VMEM((share, tokens), BF),
            pltpu.VMEM((share, tokens), BF),
            dma((5,)), dma((4,)),
            dma((10, 2)), dma((4, 3)), dma((10, nf)), dma((10,)), dma((10,)), dma((10, nf)), dma((10, nf)), dma((1,)), dma((1,)),
            dma((3, nh, nq)), dma((3, nh, nq)), dma((3, nh, nq)), dma((3, nh, nq)),
            dma((2, nh, nq)), dma((2, nh, nq)), dma((2, nh, nq)), dma((2, nh, nq)),
            dma((nq,)), dma((nq,)), dma((nq,)), dma((nq,)), dma((nt,)), dma((nt,)),
        ]
        return pl.pallas_call(
            functools.partial(staged, nr, nf, nt),
            out_shape=jax.ShapeDtypeStruct((share, tokens), BF),
            in_specs=[anywhere] * 6 + [vmem] * 4,
            out_specs=vmem,
            scratch_shapes=scratch,
            compiler_params=pltpu.CompilerParams(
                collective_id=0, has_side_effects=True, vmem_limit_bytes=60 * 1024 * 1024
            ),
        )(
            act, w_in, w_out, w_gate.T, w_up.T, w_down.T,
            *[v.reshape(-1, LANES) for v in (scale, g_mix, g_ffn, g_out)],
        )

    def on_device(act, w_in, w_out, w_gate, w_up, w_down, scale, g_mix, g_ffn, g_out):
        features, tokens = act.shape
        rows, channels = w_in.shape
        ff = w_gate.shape[1]
        share = features // nt
        nh = nt // 2
        if nr == 2 and nf == 4 and share == rows and rows % (2 * nr * LANES) == 0 and ff % (32 * nr) == 0:
            return staged_call(act, w_in, w_out, w_gate, w_up, w_down, scale, g_mix, g_ffn, g_out)
        anywhere = pl.BlockSpec(memory_space=pl.ANY)
        vmem = pl.BlockSpec(memory_space=pltpu.VMEM)
        dma = pltpu.SemaphoreType.DMA
        scratch = [
            pltpu.VMEM((nf, rows, channels), BF),
            pltpu.VMEM((nf, rows, channels), BF),
            pltpu.VMEM((nf, rows, ff), BF),
            pltpu.VMEM((nf, rows, ff), BF),
            pltpu.VMEM((nf, rows, ff), BF),
            pltpu.VMEM((features, tokens), BF),
            pltpu.VMEM((features, tokens), BF),
            pltpu.VMEM((features, tokens), BF),
            pltpu.VMEM((features, tokens), BF),
            pltpu.VMEM((channels, tokens), F32),
            pltpu.VMEM((channels, tokens), BF),
            pltpu.VMEM((ff, tokens), F32),
            pltpu.VMEM((ff, tokens), F32),
            pltpu.VMEM((ff, tokens), BF),
            pltpu.VMEM((share, tokens), F32),
            pltpu.VMEM((nt, 8, tokens), F32),
            pltpu.VMEM((2, nh, share, tokens), BF),
            pltpu.VMEM((2, nh, share, tokens), BF),
            dma((5,)),
            dma((8, 2, 2)),
            dma((8, nf)),
            dma((8, 2, 2, max(nr - 1, 1))),
            dma((8, nf, max(nr - 1, 1))),
            dma((2, nh)), dma((2, nh)), dma((2, nh)), dma((2, nh)),
            dma((nh,)), dma((nh,)), dma((nh,)), dma((nh,)),
            dma((nt,)), dma((nt,)),
        ]
        return pl.pallas_call(
            functools.partial(body, nr, nf, nt),
            out_shape=jax.ShapeDtypeStruct((share, tokens), BF),
            in_specs=[vmem] + [anywhere] * 5 + [vmem] * 4,
            out_specs=vmem,
            scratch_shapes=scratch,
            compiler_params=pltpu.CompilerParams(
                collective_id=0, has_side_effects=True, vmem_limit_bytes=60 * 1024 * 1024
            ),
        )(
            act, w_in, w_out, w_gate, w_up, w_down,
            *[v.reshape(-1, LANES) for v in (scale, g_mix, g_ffn, g_out)],
        )

    weight = P("fs", "tp")
    tokens_split = P(None, ("rep", "fs"))
    return jax.shard_map(
        on_device,
        mesh=mesh,
        in_specs=(tokens_split, *[weight] * 5, P(), P(), P(), P()),
        out_specs=P("tp", ("rep", "fs")),
        check_vma=False,
    )
```

```python
import functools

import jax
import jax.numpy as jnp
from jax import lax
from jax.experimental import pallas as pl
from jax.experimental.pallas import tpu as pltpu
from jax.sharding import PartitionSpec as P

POOL_GROUP = 256
SEQ_LEN = 256
EPS = 1e-06
LANES = 128
MESH = pl.DeviceIdType.MESH
BF = jnp.bfloat16
F32 = jnp.float32


def dot_first(weights, acts):
    return lax.dot_general(weights, acts, (((0,), (0,)), ((), ())), preferred_element_type=F32)


def column(row, width):
    square = jnp.transpose(jnp.broadcast_to(row, (LANES, LANES)))
    return jnp.concatenate([square] * (width // LANES), axis=1)


def body(
    nr, nf, nt,
    act, w_in, w_out, w_gate, w_up, w_down, scale, g_mix, g_ffn, g_out, out,
    b_in, b_out, b_gate, b_up, b_down,
    h, x1, part0, part1, u_acc, pooled, gate_acc, up_acc, hidden, own_x, squares,
    buf_a, buf_b,
    own_sem, zsend, zrecv, ysend, yrecv,
    a_send, a_recv, b_send, b_recv, c_send, c_recv, d_send, d_recv, s_send, s_recv,
):
    r, f, t = lax.axis_index("rep"), lax.axis_index("fs"), lax.axis_index("tp")
    features, tokens = act.shape
    shards = (w_in, w_out, w_gate, w_up, w_down)
    full = (b_in, b_out, b_gate, b_up, b_down)
    rows = w_in.shape[0]
    piece = rows // nr
    share = features // nt
    channels = w_in.shape[1]
    ff = w_gate.shape[1]
    nh = nt // 2
    chip, parity = t // 2, lax.rem(t, 2)
    partner = t + 1 - 2 * parity

    cut = -(-ff // (2 * LANES)) * LANES
    items = [(0, 0, channels), (1, 0, channels)]
    for m in (2, 3, 4):
        items += [(m, 0, cut), (m, cut, ff - cut)]

    own = [pltpu.make_async_copy(shards[m], full[m].at[f], own_sem.at[m]) for m in range(5)]
    for copy in own:
        copy.start()

    barrier = pltpu.get_barrier_semaphore()
    for step in (1, nf - 1):
        pl.semaphore_signal(barrier, inc=1, device_id=(r, lax.rem(f + step, nf), t), device_id_type=MESH)
    for o in range(1, nr):
        pl.semaphore_signal(barrier, inc=1, device_id=(lax.rem(r + o, nr), f, t), device_id_type=MESH)
    for i in range(1, nt):
        pl.semaphore_signal(barrier, inc=1, device_id=(r, f, lax.rem(t + i, nt)), device_id_type=MESH)
    pl.semaphore_wait(barrier, 2 + (nr - 1) + (nt - 1))

    def part_of(m, blk, of):
        matrix, start, size = items[m]
        at = pl.ds(pl.multiple_of(of * piece, piece), piece)
        return full[matrix].at[blk, at, pl.ds(start, size)]

    def z_copy(m, blk, way, d):
        ref = part_of(m, blk, r)
        return pltpu.make_async_remote_copy(
            src_ref=ref, dst_ref=ref,
            send_sem=zsend.at[m, way, lax.rem(d, 2)], recv_sem=zrecv.at[m, blk],
            device_id=(r, f + 1 - 2 * way, t), device_id_type=MESH,
        )

    def y_copy(m, blk, way, d, o):
        ref = part_of(m, blk, r)
        return pltpu.make_async_remote_copy(
            src_ref=ref, dst_ref=ref,
            send_sem=ysend.at[m, way, lax.rem(d, 2), o - 1], recv_sem=yrecv.at[m, blk, o - 1],
            device_id=(lax.rem(r + o, nr), f, t), device_id_type=MESH,
        )

    def y_arrival(m, blk, o):
        source = lax.rem(r - o + nr, nr)
        ref = part_of(m, blk, source)
        return pltpu.make_async_remote_copy(
            src_ref=ref, dst_ref=ref,
            send_sem=ysend.at[m, 0, 0, o - 1], recv_sem=yrecv.at[m, blk, o - 1],
            device_id=(lax.rem(r + o, nr), f, t), device_id_type=MESH,
        )

    can_send = (f + 1 < nf, f >= 1)
    hops = (f, nf - 1 - f)

    def send_own(m):
        if items[m][1] == 0:
            own[items[m][0]].wait()
        for way in (0, 1):
            @pl.when(can_send[way])
            def _():
                z_copy(m, f, way, 0).start()

    def arrival(m, way, d):
        blk = f - d if way == 0 else f + d

        @pl.when(d <= hops[way])
        def _():
            z_copy(m, blk, way, d).wait_recv()

            @pl.when(can_send[way])
            def _():
                @pl.when(d >= 2)
                def _():
                    z_copy(m, blk, way, d).wait_send()

                z_copy(m, blk, way, d).start()

            for o in range(1, nr):
                @pl.when(d >= 3)
                def _():
                    y_copy(m, blk, way, d, o).wait_send()

                y_copy(m, blk, way, d, o).start()

    def gather(m, low, high):
        if low >= high:
            return

        def rounds(d, carry):
            arrival(m, 0, d)
            arrival(m, 1, d)
            return carry

        if low == 1:
            rounds(jnp.int32(1), 0)
            if m + 1 < len(items):
                send_own(m + 1)
            low = 2
        lax.fori_loop(low, high, rounds, 0)

    def finish(m):
        def one(blk, carry):
            @pl.when(blk != f)
            def _():
                for o in range(1, nr):
                    y_arrival(m, blk, o).wait_recv()
            return carry

        lax.fori_loop(0, nf, one, 0)

    def drain(m):
        for way in (0, 1):
            for back in (0, 1):
                last = hops[way] - back

                @pl.when(jnp.logical_and(can_send[way], last >= 0))
                def _():
                    z_copy(m, f, way, last).wait_send()

                @pl.when(last >= 1)
                def _():
                    for o in range(1, nr):
                        y_copy(m, f, way, last, o).wait_send()

    def share_of(ref, j):
        return ref.at[pl.ds(pl.multiple_of(j * share, share), share), :]

    def normalize(load, gain, store, count):
        def square(i, total):
            v = load(i)
            return total + jnp.sum(v * v, axis=0, keepdims=True)

        total = lax.fori_loop(0, count, square, jnp.zeros((1, tokens), F32))
        factor = lax.rsqrt(total / features + EPS)

        def scaled(i, carry):
            store(i, load(i) * factor * column(gain[pl.ds(i, 1), :], tokens))
            return carry

        lax.fori_loop(0, count, scaled, 0)

    def chunk(ref, i):
        return ref[pl.ds(pl.multiple_of(i * LANES, LANES), LANES), :].astype(F32)

    def put(ref):
        def store(i, v):
            ref[pl.ds(pl.multiple_of(i * LANES, LANES), LANES), :] = v.astype(ref.dtype)
        return store

    def a_copy(k, part, c):
        return pltpu.make_async_remote_copy(
            src_ref=share_of(part, 2 * c + 1 - parity), dst_ref=buf_a.at[k, c],
            send_sem=a_send.at[k, c], recv_sem=a_recv.at[k, c],
            device_id=(r, f, partner), device_id_type=MESH,
        )

    def b_copy(k, part, i):
        target = 2 * lax.rem(chip + i, nh) + parity
        return pltpu.make_async_remote_copy(
            src_ref=share_of(part, target), dst_ref=buf_b.at[k, i],
            send_sem=b_send.at[k, i], recv_sem=b_recv.at[k, i],
            device_id=(r, f, target), device_id_type=MESH,
        )

    def start_pair(k, part):
        for i in range(nh):
            a_copy(k, part, i).start()

    def start_chips(k, part):
        for i in range(1, nh):
            c = lax.rem(chip + i, nh)
            target = 2 * c + parity
            a_copy(k, part, c).wait()

            def add(n, carry):
                at = pl.ds(pl.multiple_of(target * share + n * LANES, LANES), LANES)
                mine = part[at, :].astype(F32)
                theirs = buf_a[k, c, pl.ds(pl.multiple_of(n * LANES, LANES), LANES), :].astype(F32)
                part[at, :] = (mine + theirs).astype(BF)
                return carry

            lax.fori_loop(0, share // LANES, add, 0)
            b_copy(k, part, i).start()

    def finish_chips(k, part, base, store):
        a_copy(k, part, chip).wait()
        for i in range(1, nh):
            b_copy(k, part, i).wait()

        def add(n, carry):
            here = pl.ds(pl.multiple_of(n * LANES, LANES), LANES)
            at = pl.ds(pl.multiple_of(t * share + n * LANES, LANES), LANES)
            total = part[at, :].astype(F32) + buf_a[k, chip, here, :].astype(F32)
            for i in range(1, nh):
                total = total + buf_b[k, i, here, :].astype(F32)
            store(n, base[at, :].astype(F32) + total)
            return carry

        lax.fori_loop(0, share // LANES, add, 0)

    def c_copy(i):
        ref = share_of(x1, t)
        return pltpu.make_async_remote_copy(
            src_ref=ref, dst_ref=ref, send_sem=c_send.at[i], recv_sem=c_recv.at[i],
            device_id=(r, f, 2 * lax.rem(chip + i, nh) + parity), device_id_type=MESH,
        )

    def d_copy(i):
        ref = share_of(x1, 2 * lax.rem(chip - i + nh, nh) + parity)
        return pltpu.make_async_remote_copy(
            src_ref=ref, dst_ref=ref, send_sem=d_send.at[i], recv_sem=d_recv.at[i],
            device_id=(r, f, partner), device_id_type=MESH,
        )

    def s_copy(i):
        return pltpu.make_async_remote_copy(
            src_ref=squares.at[0], dst_ref=squares.at[i], send_sem=s_send.at[i], recv_sem=s_recv.at[i],
            device_id=(r, f, lax.rem(t + i, nt)), device_id_type=MESH,
        )

    send_own(0)
    normalize(functools.partial(chunk, act), g_mix, put(h), features // LANES)

    gather(0, 1, nf)
    gather(1, 1, nf)
    finish(0)
    u_acc[...] = jnp.zeros_like(u_acc)

    def mix_in(b, carry):
        at = pl.ds(pl.multiple_of(b * rows, rows), rows)
        u_acc[...] += dot_first(b_in[b], h[at, :])
        return carry

    lax.fori_loop(0, nf, mix_in, 0)
    for i in range(channels // LANES):
        first = t * channels + i * LANES
        window = jnp.int32(2) << (first // POOL_GROUP)
        behind = window // 2
        onward = window - behind
        source = lax.broadcasted_iota(jnp.int32, (SEQ_LEN, SEQ_LEN), 0)
        place = lax.broadcasted_iota(jnp.int32, (SEQ_LEN, SEQ_LEN), 1)
        inside = jnp.logical_and(source >= place - behind, source < place + onward)
        band = jnp.where(inside, 1.0, 0.0).astype(BF)
        spot = lax.broadcasted_iota(jnp.int32, (1, SEQ_LEN), 1)
        count = (jnp.minimum(spot + onward, SEQ_LEN) - jnp.maximum(spot - behind, 0)).astype(F32)
        gain = column(scale[pl.ds(first // LANES, 1), :], SEQ_LEN)
        for s in range(tokens // SEQ_LEN):
            at = (pl.ds(i * LANES, LANES), pl.ds(s * SEQ_LEN, SEQ_LEN))
            u = u_acc[at].astype(BF)
            mean = jnp.dot(u, band, preferred_element_type=F32) / count
            pooled[at] = ((mean - u.astype(F32)) * gain).astype(BF)

    gather(2, 1, nf)
    finish(1)

    def mix_out(b, carry):
        at = pl.ds(pl.multiple_of(b * rows, rows), rows)
        part0[at, :] = jnp.dot(b_out[b], pooled[...], preferred_element_type=F32).astype(BF)
        return carry

    lax.fori_loop(0, nf, mix_out, 0)
    start_pair(0, part0)
    gather(3, 1, nf)
    start_chips(0, part0)
    gather(4, 1, nf)

    def keep_x1(n, v):
        at = pl.ds(pl.multiple_of(t * share + n * LANES, LANES), LANES)
        x1[at, :] = v.astype(BF)

    finish_chips(0, part0, act, keep_x1)
    for i in range(1, nh):
        c_copy(i).start()
    d_copy(0).start()
    gather(5, 1, nf)
    for i in range(1, nh):
        c_copy(i).wait()
        d_copy(i).start()
    gather(6, 1, nf)
    for i in range(nh):
        d_copy(i).wait()
    normalize(functools.partial(chunk, x1), g_ffn, put(h), features // LANES)
    finish(2)
    finish(3)
    gate_acc[...] = jnp.zeros_like(gate_acc)
    up_acc[...] = jnp.zeros_like(up_acc)

    def project(source, acc):
        def one(b, carry):
            at = pl.ds(pl.multiple_of(b * rows, rows), rows)
            acc[...] += dot_first(source[b], h[at, :])
            return carry

        lax.fori_loop(0, nf, one, 0)

    gather(7, 1, nf)
    project(b_gate, gate_acc)
    finish(4)
    finish(5)
    project(b_up, up_acc)
    step = 32

    def activate(n, carry):
        at = pl.ds(pl.multiple_of(n * step, step), step)
        v = gate_acc[at, :]
        hidden[at, :] = (v / (1.0 + jnp.exp(-v)) * up_acc[at, :]).astype(BF)
        return carry

    lax.fori_loop(0, ff // step, activate, 0)
    finish(6)
    finish(7)

    def mlp_out(b, carry):
        at = pl.ds(pl.multiple_of(b * rows, rows), rows)
        part1[at, :] = jnp.dot(b_down[b], hidden[...], preferred_element_type=F32).astype(BF)
        return carry

    if share % rows == 0:
        blocks = share // rows

        def pair_out(c):
            theirs, ours = 2 * c + 1 - parity, 2 * c + parity
            lax.fori_loop(theirs * blocks, (theirs + 1) * blocks, mlp_out, 0)
            a_copy(1, part1, c).start()
            lax.fori_loop(ours * blocks, (ours + 1) * blocks, mlp_out, 0)

        for i in range(1, nh):
            pair_out(lax.rem(chip + i, nh))
        start_chips(1, part1)
        pair_out(chip)
    else:
        lax.fori_loop(0, nf, mlp_out, 0)
        start_pair(1, part1)
        start_chips(1, part1)
    for m in range(len(items)):
        drain(m)
    finish_chips(1, part1, x1, put(own_x))

    def square(i, total):
        v = chunk(own_x, i)
        return total + jnp.sum(v * v, axis=0, keepdims=True)

    mine = lax.fori_loop(0, share // LANES, square, jnp.zeros((1, tokens), F32))
    squares[0] = jnp.broadcast_to(mine, squares.shape[1:])
    for i in range(1, nt):
        s_copy(i).start()
    for i in range(1, nt):
        s_copy(i).wait()
    total = squares[0, pl.ds(0, 1), :]
    for i in range(1, nt):
        total = total + squares[i, pl.ds(0, 1), :]
    factor = lax.rsqrt(total / features + EPS)

    def closing(i, carry):
        gain = column(g_out[pl.ds(t * (share // LANES) + i, 1), :], tokens)
        put(out)(i, chunk(own_x, i) * factor * gain)
        return carry

    lax.fori_loop(0, share // LANES, closing, 0)


def staged(
    nr, nf, nt,
    act, w_in, w_out, w_gate, w_up, w_down, scale, g_mix, g_ffn, g_out, out,
    b_in, b_out, b_gate, b_up, b_down,
    x0, h, x1, part, pooled, gate_acc, up_acc, hidden, own_x, squares, power,
    buf_a, buf_b, back, home,
    own_sem, act_sem, in_send, out_send, zrecv, wrecv, ysend, yrecv, v_send, v_recv,
    a_send, a_recv, b_send, b_recv, c_send, c_recv, d_send, d_recv,
    e_send, e_recv, g_send, g_recv, s_send, s_recv,
):
    r, f, t = lax.axis_index("rep"), lax.axis_index("fs"), lax.axis_index("tp")
    features, tokens = act.shape
    shards = (w_in, w_out, w_gate, w_up, w_down)
    full = (b_in, b_out, b_gate, b_up, b_down)
    rows, channels = w_in.shape
    ff = w_gate.shape[0]
    share = features // nt
    nh = nt // 2
    nq = share // LANES
    chip, parity = t // 2, lax.rem(t, 2)
    partner = t + 1 - 2 * parity
    other_rep = lax.rem(r + 1, nr)
    cuts = 2
    slab = share // cuts
    items = [(0, 0), (0, 1), (1, 0), (1, 1), (2, 0), (3, 0), (2, 1), (3, 1), (4, 0), (4, 1)]
    early = 4
    extra = 7
    last = len(items)
    left = f < nf // 2
    inner = jnp.logical_and(f >= 1, f < nf - 1)
    outer = jnp.logical_not(inner)
    mate = jnp.where(left, 1 - f, 2 * nf - 3 - f)
    inward = jnp.where(left, f + 1, f - 1)
    over = jnp.where(inner, nf - 1 - f, nf - 1 - mate)
    far = jnp.where(inner, nf - 1 - mate, nf - 1 - f)
    blocks = (mate, over, far)

    own = [pltpu.make_async_copy(shards[m], full[m].at[f], own_sem.at[m]) for m in range(5)]
    stream = [pltpu.make_async_copy(act, x0, act_sem.at[0])]
    own[0].start()
    own[1].start()
    for copy in stream:
        copy.start()
    for copy in own[2:]:
        copy.start()

    barrier = pltpu.get_barrier_semaphore()
    for step in (1, nf - 1):
        pl.semaphore_signal(barrier, inc=1, device_id=(r, lax.rem(f + step, nf), t), device_id_type=MESH)
    pl.semaphore_signal(barrier, inc=1, device_id=(other_rep, f, t), device_id_type=MESH)
    for i in range(1, nt):
        pl.semaphore_signal(barrier, inc=1, device_id=(r, f, lax.rem(t + i, nt)), device_id_type=MESH)
    pl.semaphore_wait(barrier, 3 + (nt - 1))

    def line(start, size=LANES):
        return pl.ds(pl.multiple_of(start, size), size)

    def part_of(m, blk, of):
        matrix, s = items[m]
        if matrix < 2:
            size = rows // cuts // nr
            return full[matrix].at[blk, line((s * nr + of) * size, size), :]
        if matrix < 4:
            size = ff // cuts // nr
            return full[matrix].at[blk, line((s * nr + of) * size, size), :]
        size = rows // cuts // nr
        return full[matrix].at[blk, :, line((s * nr + of) * size, size)]

    def remote(ref, dst, send, recv, device):
        return pltpu.make_async_remote_copy(
            src_ref=ref, dst_ref=dst, send_sem=send, recv_sem=recv, device_id=device, device_id_type=MESH
        )

    def group(m):
        return max(items[m][0] - 1, 0)

    def in_copy(m, blk, d):
        ref = part_of(m, blk, r)
        place = jnp.where(inner, 1, 0) if d == 0 else 2
        return remote(ref, ref, in_send.at[group(m)], zrecv.at[m, place], (r, inward, t))

    def out_copy(m, blk, j):
        ref = part_of(m, blk, r)
        return remote(ref, ref, out_send.at[0], zrecv.at[m, j], (r, mate, t))

    def arrive(m, j):
        ref = part_of(m, blocks[j], r)
        remote(ref, ref, in_send.at[group(m)], zrecv.at[m, j], (r, mate, t)).wait_recv()

    def lot(m):
        return (m - early) // 2 if m < 2 * cuts + early else m - early - cuts

    def w_copy(m, blk):
        ref = part_of(m, blk, other_rep)
        return remote(ref, ref, in_send.at[group(m)], wrecv.at[lot(m)], (r, mate, t))

    def v_copy(blk):
        ref = part_of(extra, blk, other_rep)
        return remote(ref, ref, v_send.at[0], v_recv.at[0], (r, inward, t))

    def y_copy(m, j, of):
        ref = part_of(m, blocks[j], of)
        place = m // 2 if m < last - 2 else last // 2 + 2 * (m - last + 2) + j - 2
        return remote(ref, ref, ysend.at[group(m)], yrecv.at[place], (other_rep, f, t))

    def y_lot(ref, place):
        return remote(ref, ref, ysend.at[0], yrecv.at[place], (other_rep, f, t))

    def own_ready(m):
        if items[m][1] == 0:
            own[items[m][0]].wait()

    def send_mixer(m):
        own_ready(m)
        in_copy(m, f, 0).start()

        @pl.when(inner)
        def _():
            out_copy(m, f, 0).start()

    def hop(m, j):
        arrive(m, j)
        if j == 0:
            in_copy(m, mate, 1).start()
        else:
            out_copy(m, blocks[j], j).start()

    def side(m, j):
        y_copy(m, j, r).start()

    def relay(m, j):
        hop(m, j)
        side(m, j)

    def collect(m, j):
        arrive(m, j)
        side(m, j)

    def y_arrival(m, j):
        y_copy(m, j, other_rep).wait_recv()

    def finish(matrix):
        y_lot(full[matrix].at[pl.ds(0, nf - 1), pl.ds(0, rows // nr)], matrix).wait_recv()

    def send_inner(m):
        in_copy(m, f, 0).start()

    def send_outer(m):
        in_copy(m, f, 0).start()
        w_copy(m, f).start()

    def pass_on(m):
        hop(m, 0)

    def cross(m, *some):
        for j in some:
            arrive(m, j)
            if m != extra or j == 2:
                side(m, j)

    def settle(s):
        ref = full[2].at[0, pl.ds(0, ff // cuts)]
        remote(ref, ref, in_send.at[1], wrecv.at[s], (r, mate, t)).wait_recv()
        pieces = 2 * nr - (s == cuts - 1)
        y_lot(full[2].at[0, pl.ds(0, pieces * (ff // cuts // nr))], 2 + s).wait_recv()
        if s == cuts - 1:
            v_copy(over).wait_recv()

    def spot(target, q, size=LANES):
        return line(target * share + q * size, size)

    def normalize(load, gain, store, count):
        def square(i, total):
            v = load(i)
            return total + jnp.sum(v * v, axis=0, keepdims=True)

        total = lax.fori_loop(0, count, square, jnp.zeros((1, tokens), F32))
        factor = lax.rsqrt(total / features + EPS)

        def scaled(i, carry):
            store(i, load(i) * factor * column(gain[pl.ds(i, 1), :], tokens))
            return carry

        lax.fori_loop(0, count, scaled, 0)

    def chunk(ref, i):
        return ref[line(i * LANES), :].astype(F32)

    def put(ref):
        def store(i, v):
            ref[line(i * LANES), :] = v.astype(ref.dtype)
        return store

    def a_copy(k, target, q, size):
        return remote(
            part.at[k, spot(target, q, size)], buf_a.at[k, target // 2, line(q * size, size)],
            a_send.at[k], a_recv.at[k, target // 2, q], (r, f, partner),
        )

    def b_copy(k, i, q, size):
        target = 2 * lax.rem(chip + i, nh) + parity
        return remote(
            part.at[k, spot(target, q, size)], buf_b.at[k, i, line(q * size, size)],
            b_send.at[k], b_recv.at[k, i - 1, q], (r, f, target),
        )

    def c_copy(k, i, q):
        ref = x1.at[k, spot(t, q)]
        device = (r, f, 2 * lax.rem(chip + i, nh) + parity)
        return remote(ref, ref, c_send.at[k], c_recv.at[k, i - 1, q], device)

    def d_copy(k, i, q):
        ref = x1.at[k, spot(2 * lax.rem(chip - i + nh, nh) + parity, q)]
        return remote(ref, ref, d_send.at[k], d_recv.at[k, i], (r, f, partner))

    def e_copy(q):
        return remote(x1.at[0, spot(t, q)], x1.at[1, spot(t, q)], e_send.at[0], e_recv.at[q], (r, mate, t))

    def g_copy(q):
        return remote(back.at[line(q * LANES)], home.at[line(q * LANES)], g_send.at[0], g_recv.at[q], (r, mate, t))

    def s_copy(i):
        return remote(squares.at[0], squares.at[i], s_send.at[0], s_recv.at[0], (r, f, lax.rem(t + i, nt)))

    def add_pair(k, target, q, size):
        for n in range(size // LANES):
            here = line(q * size + n * LANES)
            at = line(target * share + q * size + n * LANES)
            mine, theirs = part[k, at, :].astype(F32), buf_a[k, target // 2, here, :].astype(F32)
            part[k, at, :] = (mine + theirs).astype(BF)

    def total_of(k, q):
        here = line(q * LANES)
        total = part[k, spot(t, q), :].astype(F32) + buf_a[k, chip, here, :].astype(F32)
        for i in range(1, nh):
            total = total + buf_b[k, i, here, :].astype(F32)
        return total

    send_mixer(0)
    send_mixer(1)
    for m in (2, 4, 5, 8):
        own_ready(m)

    @pl.when(outer)
    def _():
        for m in (2, 3):
            in_copy(m, f, 0).start()
        for m in (4, 5, 6):
            send_outer(m)
        in_copy(7, f, 0).start()

    @pl.when(inner)
    def _():
        in_copy(2, f, 0).start()

    for copy in stream:
        copy.wait()
    normalize(functools.partial(chunk, x0), g_mix, put(h.at[0]), features // LANES)

    @pl.when(inner)
    def _():
        relay(0, 0)
        relay(0, 1)
        relay(1, 0)
        relay(1, 1)
        in_copy(3, f, 0).start()
        hop(2, 0)
        hop(3, 0)
        send_inner(4)
        for m in (2, 3):
            out_copy(m, f, 0).start()
        relay(0, 2)
        relay(1, 2)
        side(2, 0)
        side(3, 0)
        relay(2, 1)
        relay(3, 1)
        pass_on(4)
        send_inner(5)

    @pl.when(outer)
    def _():
        for j in range(3):
            collect(0, j)
            collect(1, j)

    finish(0)

    u_mix = dot_first(b_in[0], h[0, pl.ds(0, rows), :])
    for b in range(1, nf):
        u_mix += dot_first(b_in[b], h[0, pl.ds(b * rows, rows), :])
    gate_acc[pl.ds(0, channels), :] = u_mix
    for i in range(channels // LANES):
        first = t * channels + i * LANES
        window = jnp.int32(2) << (first // POOL_GROUP)
        behind = window // 2
        onward = window - behind
        source = lax.broadcasted_iota(jnp.int32, (SEQ_LEN, SEQ_LEN), 0)
        place = lax.broadcasted_iota(jnp.int32, (SEQ_LEN, SEQ_LEN), 1)
        inside = jnp.logical_and(source >= place - behind, source < place + onward)
        band = jnp.where(inside, 1.0, 0.0).astype(BF)
        seat = lax.broadcasted_iota(jnp.int32, (1, SEQ_LEN), 1)
        count = (jnp.minimum(seat + onward, SEQ_LEN) - jnp.maximum(seat - behind, 0)).astype(F32)
        gain = column(scale[pl.ds(first // LANES, 1), :], SEQ_LEN)
        for s in range(tokens // SEQ_LEN):
            at = (pl.ds(i * LANES, LANES), pl.ds(s * SEQ_LEN, SEQ_LEN))
            u = gate_acc[at].astype(BF)
            mean = jnp.dot(u, band, preferred_element_type=F32) / count
            pooled[at] = ((mean - u.astype(F32)) * gain).astype(BF)

    mixed = True

    @pl.when(inner)
    def _():
        relay(2, 2)
        relay(3, 2)
        cross(4, 1)
        pass_on(5)
        send_inner(6)
        cross(4, 2)

    @pl.when(outer)
    def _():
        for j in range(3):
            collect(2, j)
            collect(3, j)

    finish(1)

    def mix_out(target):
        part[0, line(target * share, share), :] = jnp.dot(
            b_out[target], pooled[...], preferred_element_type=F32
        ).astype(BF)

    for i in range(1, nh + 1):
        c = lax.rem(chip + i, nh)
        mix_out(2 * c + 1 - parity)
        a_copy(0, 2 * c + 1 - parity, 0, share).start()
        mix_out(2 * c + parity)
    for i in range(1, nh):
        target = 2 * lax.rem(chip + i, nh) + parity
        a_copy(0, target, 0, share).wait_recv()
        for q in range(nq):
            add_pair(0, target, q, LANES)
            b_copy(0, i, q, LANES).start()
    a_copy(0, t, 0, share).wait_recv()

    @pl.when(inner)
    def _():
        cross(5, 1)

    def prepare(k, target, q):
        at = spot(target, q)
        v = x1[k, at, :].astype(F32)
        h[k, at, :] = (v * column(g_ffn[pl.ds(target * nq + q, 1), :], tokens)).astype(BF)
        power[k] += jnp.sum((v * v).reshape(LANES // 8, 8, tokens), axis=0)

    power[...] = jnp.zeros_like(power)

    for q in range(nq):
        for i in range(1, nh):
            b_copy(0, i, q, LANES).wait_recv()
        x1[0, spot(t, q), :] = (x0[spot(t, q), :].astype(F32) + total_of(0, q)).astype(BF)

        @pl.when(inner)
        def _():
            for i in range(1, nh):
                c_copy(0, i, q).start()
            d_copy(0, 0, q).start()
            prepare(0, t, q)
            if q == 0:
                pass_on(6)
                send_inner(7)
                cross(5, 2)
            if q == 1:
                cross(6, 1)
            if q == 2:
                pass_on(7)
                send_inner(8)
                v_copy(f).start()
                send_inner(9)

        @pl.when(outer)
        def _():
            e_copy(q).start()

    cut = ff // cuts
    step = 32
    wide = 2 * LANES

    def project(k, s, targets, fresh):
        at = pl.ds(s * cut, cut)
        for source, acc in ((b_gate, gate_acc), (b_up, up_acc)):
            def tokens_at(n, carry):
                here = line(n * wide, wide)
                terms = [
                    jnp.dot(source[b, at, :], h[k, line(b * rows, rows), here], preferred_element_type=F32)
                    for b in targets
                ]
                total = functools.reduce(lambda x, y: x + y, terms)
                acc[at, here] = total if fresh else acc[at, here] + total
                return carry

            lax.fori_loop(0, tokens // wide, tokens_at, 0)

    def activate(k, s):
        total = jnp.sum(power[k], axis=0, keepdims=True)
        factor = lax.rsqrt(total / features + EPS)

        def some(n, carry):
            here = line(s * cut + n * step, step)
            v = gate_acc[here, :] * factor
            hidden[k, here, :] = (v / (1.0 + jnp.exp(-v)) * (up_acc[here, :] * factor)).astype(BF)
            return carry

        lax.fori_loop(0, cut // step, some, 0)

    def mlp_out(k, target, s):
        at = spot(target, s, slab)
        part[1 + k, at, :] = dot_first(b_down[target, :, line(s * slab, slab)], hidden[k]).astype(BF)

        @pl.when(lax.rem(target, 2) != parity)
        def _():
            a_copy(1 + k, target, s, slab).start()

    def pair_up(k, target, s):
        @pl.when(lax.rem(target, 2) == parity)
        def _():
            a_copy(1 + k, target, s, slab).wait_recv()
            for i in range(1, nh):
                @pl.when(target // 2 == lax.rem(chip + i, nh))
                def _():
                    add_pair(1 + k, target, s, slab)
                    b_copy(1 + k, i, s, slab).start()

    plans = (
        [(1, 2, 0), (1, 3, 0), (1, 0, 0), (1, 1, 0), (1, 2, 1), (1, 3, 1), (1, 0, 1), (1, 1, 1),
         (0, 2, 1), (0, 3, 0), (0, 3, 1), (0, 0, 0), (0, 0, 1), (0, 1, 0), (0, 1, 1)],
        [(1, 0, 0), (1, 1, 0), (1, 2, 0), (1, 3, 0), (1, 0, 1), (1, 1, 1), (1, 2, 1), (1, 3, 1),
         (0, 0, 1), (0, 1, 0), (0, 1, 1), (0, 2, 0), (0, 3, 0), (0, 2, 1), (0, 3, 1)],
    )
    near = chip == f // 2

    def planned(n):
        k, s, target = jnp.int32(0), jnp.int32(0), f
        for plan, taken in zip(plans, (near, jnp.logical_not(near))):
            for at, (kk, code, ss) in enumerate(plan):
                here = jnp.logical_and(n == at, taken)
                k = jnp.where(here, kk, k)
                s = jnp.where(here, ss, s)
                target = jnp.where(here, (f, mate, over, far)[code], target)
        return k, target, s

    def give_back(s):
        for i in range(1, nh):
            b_copy(2, i, s, slab).wait_recv()
        for n in range(slab // LANES):
            q = s * (slab // LANES) + n
            back[pl.ds(q * LANES, LANES), :] = total_of(2, q).astype(BF)
            g_copy(q).start()

    def spread(q):
        e_copy(q).wait_recv()
        for i in range(1, nh):
            c_copy(1, i, q).start()
        d_copy(1, 0, q).start()
        prepare(1, t, q)

    def mine(i):
        return 2 * lax.rem(chip - i + nh, nh) + parity

    def theirs(i):
        return 2 * lax.rem(chip - i + nh, nh) + 1 - parity

    def hand_over(k, q):
        for i in range(1, nh):
            c_copy(k, i, q).wait_recv()
            d_copy(k, i, q).start()
            prepare(k, mine(i), q)

    def absorb(k, i):
        ref = x1.at[k, line(theirs(i) * share, share)]
        remote(ref, ref, d_send.at[k], d_recv.at[k, i], (r, f, partner)).wait_recv()
        for q in range(nq):
            prepare(k, theirs(i), q)

    here_blocks = (t, partner)
    away_blocks = tuple(b for i in range(1, nh) for b in (mine(i), theirs(i)))

    @pl.when(inner)
    def _():
        cross(6, 2)
        absorb(0, 0)
        hand_over(0, 0)
        cross(7, 1)
        hand_over(0, 1)
        spread(0)
        cross(7, 2)
        hand_over(0, 2)
        spread(1)
        cross(8, 1)
        hand_over(0, 3)
        spread(2)
        spread(3)
        for i in range(1, nh):
            absorb(0, i)
        settle(0)
        project(0, 0, here_blocks + away_blocks, True)
        activate(0, 0)
        hand_over(1, 0)
        settle(1)
        project(0, 1, here_blocks + away_blocks, True)
        activate(0, 1)
        pass_on(8)
        hand_over(1, 1)

        @pl.when(near)
        def _():
            y_arrival(8, 1)

        lead = jnp.where(near, over, f)
        mlp_out(0, lead, 0)

        absorb(1, 0)
        project(1, 0, here_blocks, True)
        hand_over(1, 2)
        cross(9, 1)
        pair_up(0, lead, 0)
        pass_on(9)
        project(1, 1, here_blocks, True)
        cross(8, 2)
        hand_over(1, 3)
        for i in range(1, nh):
            absorb(1, i)
        project(1, 0, away_blocks, False)
        activate(1, 0)
        project(1, 1, away_blocks, False)
        activate(1, 1)
        cross(9, 2)

        def ffn(n, carry):
            near_waits = (
                (1, lambda: y_arrival(8, 2)),
                (3, lambda: w_copy(8, mate).wait_recv()),
                (4, lambda: y_arrival(9, 1)),
                (5, lambda: y_arrival(9, 2)),
                (7, lambda: w_copy(9, mate).wait_recv()),
            )
            away_waits = (
                (1, lambda: w_copy(8, mate).wait_recv()),
                (2, lambda: y_arrival(8, 1)),
                (3, lambda: y_arrival(8, 2)),
                (5, lambda: w_copy(9, mate).wait_recv()),
                (6, lambda: y_arrival(9, 1)),
                (7, lambda: y_arrival(9, 2)),
            )
            for waits, taken in ((near_waits, near), (away_waits, jnp.logical_not(near))):
                for at, wait in waits:
                    @pl.when(jnp.logical_and(n == at, taken))
                    def _():
                        wait()

            @pl.when(n == 10)
            def _():
                give_back(0)

            mlp_out(*planned(n))

            @pl.when(n >= 1)
            def _():
                pair_up(*planned(n - 1))
            return carry

        lax.fori_loop(0, len(plans[0]), ffn, 0)
        pair_up(*planned(len(plans[0]) - 1))
        give_back(1)
        for q in range(nq):
            for i in range(1, nh):
                if q % (slab // LANES) == 0:
                    b_copy(1, i, q // (slab // LANES), slab).wait_recv()
            own_x[pl.ds(q * LANES, LANES), :] = x1[0, spot(t, q), :].astype(F32) + total_of(1, q)

    @pl.when(outer)
    def _():
        w_copy(7, f).start()
        for m in (8, 9):
            in_copy(m, f, 0).start()
        for m in (8, 9):
            w_copy(m, f).start()
        for q in range(nq):
            g_copy(q).wait_recv()
            at = pl.ds(q * LANES, LANES)
            own_x[at, :] = x1[0, spot(t, q), :].astype(F32) + home[at, :].astype(F32)

    total = jnp.zeros((1, tokens), F32)
    for q in range(nq):
        v = own_x[pl.ds(q * LANES, LANES), :]
        total += jnp.sum(v * v, axis=0, keepdims=True)
    squares[0] = jnp.broadcast_to(total, squares.shape[1:])
    for i in range(1, nt):
        s_copy(i).start()

    got = squares.at[pl.ds(1, nt - 1)]
    remote(got, got, s_send.at[0], s_recv.at[0], (r, f, partner)).wait_recv()
    for i in range(1, nt):
        total = total + squares[i, pl.ds(0, 1), :]
    factor = lax.rsqrt(total / features + EPS)

    def closing(q):
        gain = column(g_out[pl.ds(t * nq + q, 1), :], tokens)
        out[pl.ds(q * LANES, LANES), :] = (own_x[pl.ds(q * LANES, LANES), :] * factor * gain).astype(BF)

    for q in range(nq):
        closing(q)

    def sent(ref, sem):
        remote(ref, ref, sem, zrecv.at[0, 0], (r, mate, t)).wait_send()

    for matrix in (2, 3, 4):
        sent(full[matrix].at[0], in_send.at[matrix - 1])
    sent(full[0].at[pl.ds(0, nf - 1)], ysend.at[0])
    sent(part.at[0, pl.ds(0, nh * share)], a_send.at[0])
    sent(part.at[0, pl.ds(0, (nh - 1) * share)], b_send.at[0])
    sent(squares.at[pl.ds(1, nt - 1)], s_send.at[0])

    @pl.when(inner)
    def _():
        sent(full[0].at[pl.ds(0, 2)], in_send.at[0])
        sent(full[0].at[pl.ds(0, nf - 1)], out_send.at[0])
        v_copy(f).wait_send()
        sent(full[2].at[0], ysend.at[1])
        sent(full[3].at[0, pl.ds(0, (2 * nr - 1) * (ff // cuts // nr))], ysend.at[2])
        sent(full[4].at[0], ysend.at[3])
        for k in (0, 1):
            sent(part.at[0, pl.ds(0, nh * share)], a_send.at[1 + k])
            sent(part.at[0, pl.ds(0, (nh - 1) * share)], b_send.at[1 + k])
            sent(part.at[0, pl.ds(0, nh * share)], d_send.at[k])
            sent(part.at[0, pl.ds(0, (nh - 1) * share)], c_send.at[k])
        sent(back, g_send.at[0])

    @pl.when(outer)
    def _():
        sent(full[0].at[0], in_send.at[0])
        sent(back, e_send.at[0])


def solution(mesh):
    nr, nf, nt = mesh.shape["rep"], mesh.shape["fs"], mesh.shape["tp"]

    def staged_call(act, w_in, w_out, w_gate, w_up, w_down, scale, g_mix, g_ffn, g_out):
        features, tokens = act.shape
        rows, channels = w_in.shape
        ff = w_gate.shape[1]
        share = features // nt
        nh = nt // 2
        nq = share // LANES
        anywhere = pl.BlockSpec(memory_space=pl.ANY)
        vmem = pl.BlockSpec(memory_space=pltpu.VMEM)
        dma = pltpu.SemaphoreType.DMA
        scratch = [
            pltpu.VMEM((nf, rows, channels), BF),
            pltpu.VMEM((nf, rows, channels), BF),
            pltpu.VMEM((nf, ff, rows), BF),
            pltpu.VMEM((nf, ff, rows), BF),
            pltpu.VMEM((nf, ff, rows), BF),
            pltpu.VMEM((features, tokens), BF),
            pltpu.VMEM((2, features, tokens), BF),
            pltpu.VMEM((2, features, tokens), BF),
            pltpu.VMEM((3, features, tokens), BF),
            pltpu.VMEM((channels, tokens), BF),
            pltpu.VMEM((ff, tokens), F32),
            pltpu.VMEM((ff, tokens), F32),
            pltpu.VMEM((2, ff, tokens), BF),
            pltpu.VMEM((share, tokens), F32),
            pltpu.VMEM((nt, 8, tokens), F32),
            pltpu.VMEM((2, 8, tokens), F32),
            pltpu.VMEM((3, nh, share, tokens), BF),
            pltpu.VMEM((3, nh, share, tokens), BF),
            pltpu.VMEM((share, tokens), BF),
            pltpu.VMEM((share, tokens), BF),
            dma((5,)), dma((1,)),
            dma((4,)), dma((1,)), dma((10, 3)), dma((4,)), dma((4,)), dma((8,)), dma((1,)), dma((1,)),
            dma((3,)), dma((3, nh, 2)), dma((3,)), dma((3, nh - 1, nq)),
            dma((2,)), dma((2, nh - 1, nq)), dma((2,)), dma((2, nh)),
            dma((1,)), dma((nq,)), dma((1,)), dma((nq,)), dma((1,)), dma((1,)),
        ]
        return pl.pallas_call(
            functools.partial(staged, nr, nf, nt),
            out_shape=jax.ShapeDtypeStruct((share, tokens), BF),
            in_specs=[anywhere] * 6 + [vmem] * 4,
            out_specs=vmem,
            scratch_shapes=scratch,
            compiler_params=pltpu.CompilerParams(
                collective_id=0, has_side_effects=True, vmem_limit_bytes=60 * 1024 * 1024
            ),
        )(
            act, w_in, w_out, w_gate.T, w_up.T, w_down.T,
            *[v.reshape(-1, LANES) for v in (scale, g_mix, g_ffn, g_out)],
        )

    def on_device(act, w_in, w_out, w_gate, w_up, w_down, scale, g_mix, g_ffn, g_out):
        features, tokens = act.shape
        rows, channels = w_in.shape
        ff = w_gate.shape[1]
        share = features // nt
        nh = nt // 2
        if nr == 2 and nf == 4 and share == rows and rows % (2 * nr * LANES) == 0 and ff % (32 * nr) == 0:
            return staged_call(act, w_in, w_out, w_gate, w_up, w_down, scale, g_mix, g_ffn, g_out)
        anywhere = pl.BlockSpec(memory_space=pl.ANY)
        vmem = pl.BlockSpec(memory_space=pltpu.VMEM)
        dma = pltpu.SemaphoreType.DMA
        scratch = [
            pltpu.VMEM((nf, rows, channels), BF),
            pltpu.VMEM((nf, rows, channels), BF),
            pltpu.VMEM((nf, rows, ff), BF),
            pltpu.VMEM((nf, rows, ff), BF),
            pltpu.VMEM((nf, rows, ff), BF),
            pltpu.VMEM((features, tokens), BF),
            pltpu.VMEM((features, tokens), BF),
            pltpu.VMEM((features, tokens), BF),
            pltpu.VMEM((features, tokens), BF),
            pltpu.VMEM((channels, tokens), F32),
            pltpu.VMEM((channels, tokens), BF),
            pltpu.VMEM((ff, tokens), F32),
            pltpu.VMEM((ff, tokens), F32),
            pltpu.VMEM((ff, tokens), BF),
            pltpu.VMEM((share, tokens), F32),
            pltpu.VMEM((nt, 8, tokens), F32),
            pltpu.VMEM((2, nh, share, tokens), BF),
            pltpu.VMEM((2, nh, share, tokens), BF),
            dma((5,)),
            dma((8, 2, 2)),
            dma((8, nf)),
            dma((8, 2, 2, max(nr - 1, 1))),
            dma((8, nf, max(nr - 1, 1))),
            dma((2, nh)), dma((2, nh)), dma((2, nh)), dma((2, nh)),
            dma((nh,)), dma((nh,)), dma((nh,)), dma((nh,)),
            dma((nt,)), dma((nt,)),
        ]
        return pl.pallas_call(
            functools.partial(body, nr, nf, nt),
            out_shape=jax.ShapeDtypeStruct((share, tokens), BF),
            in_specs=[vmem] + [anywhere] * 5 + [vmem] * 4,
            out_specs=vmem,
            scratch_shapes=scratch,
            compiler_params=pltpu.CompilerParams(
                collective_id=0, has_side_effects=True, vmem_limit_bytes=60 * 1024 * 1024
            ),
        )(
            act, w_in, w_out, w_gate, w_up, w_down,
            *[v.reshape(-1, LANES) for v in (scale, g_mix, g_ffn, g_out)],
        )

    weight = P("fs", "tp")
    tokens_split = P(None, ("rep", "fs"))
    return jax.shard_map(
        on_device,
        mesh=mesh,
        in_specs=(tokens_split, *[weight] * 5, P(), P(), P(), P()),
        out_specs=P("tp", ("rep", "fs")),
        check_vma=False,
    )
```

```python
import functools

import jax
import jax.numpy as jnp
from jax import lax
from jax.experimental import pallas as pl
from jax.experimental.pallas import tpu as pltpu
from jax.sharding import PartitionSpec as P

POOL_GROUP = 256
SEQ_LEN = 256
EPS = 1e-06
LANES = 128
MESH = pl.DeviceIdType.MESH
BF = jnp.bfloat16
F32 = jnp.float32


def dot_first(weights, acts):
    return lax.dot_general(weights, acts, (((0,), (0,)), ((), ())), preferred_element_type=F32)


def column(row, width):
    square = jnp.transpose(jnp.broadcast_to(row, (LANES, LANES)))
    return jnp.concatenate([square] * (width // LANES), axis=1)


def body(
    nr, nf, nt,
    act, w_in, w_out, w_gate, w_up, w_down, scale, g_mix, g_ffn, g_out, out,
    b_in, b_out, b_gate, b_up, b_down,
    h, x1, part0, part1, u_acc, pooled, gate_acc, up_acc, hidden, own_x, squares,
    buf_a, buf_b,
    own_sem, zsend, zrecv, ysend, yrecv,
    a_send, a_recv, b_send, b_recv, c_send, c_recv, d_send, d_recv, s_send, s_recv,
):
    r, f, t = lax.axis_index("rep"), lax.axis_index("fs"), lax.axis_index("tp")
    features, tokens = act.shape
    shards = (w_in, w_out, w_gate, w_up, w_down)
    full = (b_in, b_out, b_gate, b_up, b_down)
    rows = w_in.shape[0]
    piece = rows // nr
    share = features // nt
    channels = w_in.shape[1]
    ff = w_gate.shape[1]
    nh = nt // 2
    chip, parity = t // 2, lax.rem(t, 2)
    partner = t + 1 - 2 * parity

    cut = -(-ff // (2 * LANES)) * LANES
    items = [(0, 0, channels), (1, 0, channels)]
    for m in (2, 3, 4):
        items += [(m, 0, cut), (m, cut, ff - cut)]

    own = [pltpu.make_async_copy(shards[m], full[m].at[f], own_sem.at[m]) for m in range(5)]
    for copy in own:
        copy.start()

    barrier = pltpu.get_barrier_semaphore()
    for step in (1, nf - 1):
        pl.semaphore_signal(barrier, inc=1, device_id=(r, lax.rem(f + step, nf), t), device_id_type=MESH)
    for o in range(1, nr):
        pl.semaphore_signal(barrier, inc=1, device_id=(lax.rem(r + o, nr), f, t), device_id_type=MESH)
    for i in range(1, nt):
        pl.semaphore_signal(barrier, inc=1, device_id=(r, f, lax.rem(t + i, nt)), device_id_type=MESH)
    pl.semaphore_wait(barrier, 2 + (nr - 1) + (nt - 1))

    def part_of(m, blk, of):
        matrix, start, size = items[m]
        at = pl.ds(pl.multiple_of(of * piece, piece), piece)
        return full[matrix].at[blk, at, pl.ds(start, size)]

    def z_copy(m, blk, way, d):
        ref = part_of(m, blk, r)
        return pltpu.make_async_remote_copy(
            src_ref=ref, dst_ref=ref,
            send_sem=zsend.at[m, way, lax.rem(d, 2)], recv_sem=zrecv.at[m, blk],
            device_id=(r, f + 1 - 2 * way, t), device_id_type=MESH,
        )

    def y_copy(m, blk, way, d, o):
        ref = part_of(m, blk, r)
        return pltpu.make_async_remote_copy(
            src_ref=ref, dst_ref=ref,
            send_sem=ysend.at[m, way, lax.rem(d, 2), o - 1], recv_sem=yrecv.at[m, blk, o - 1],
            device_id=(lax.rem(r + o, nr), f, t), device_id_type=MESH,
        )

    def y_arrival(m, blk, o):
        source = lax.rem(r - o + nr, nr)
        ref = part_of(m, blk, source)
        return pltpu.make_async_remote_copy(
            src_ref=ref, dst_ref=ref,
            send_sem=ysend.at[m, 0, 0, o - 1], recv_sem=yrecv.at[m, blk, o - 1],
            device_id=(lax.rem(r + o, nr), f, t), device_id_type=MESH,
        )

    can_send = (f + 1 < nf, f >= 1)
    hops = (f, nf - 1 - f)

    def send_own(m):
        if items[m][1] == 0:
            own[items[m][0]].wait()
        for way in (0, 1):
            @pl.when(can_send[way])
            def _():
                z_copy(m, f, way, 0).start()

    def arrival(m, way, d):
        blk = f - d if way == 0 else f + d

        @pl.when(d <= hops[way])
        def _():
            z_copy(m, blk, way, d).wait_recv()

            @pl.when(can_send[way])
            def _():
                @pl.when(d >= 2)
                def _():
                    z_copy(m, blk, way, d).wait_send()

                z_copy(m, blk, way, d).start()

            for o in range(1, nr):
                @pl.when(d >= 3)
                def _():
                    y_copy(m, blk, way, d, o).wait_send()

                y_copy(m, blk, way, d, o).start()

    def gather(m, low, high):
        if low >= high:
            return

        def rounds(d, carry):
            arrival(m, 0, d)
            arrival(m, 1, d)
            return carry

        if low == 1:
            rounds(jnp.int32(1), 0)
            if m + 1 < len(items):
                send_own(m + 1)
            low = 2
        lax.fori_loop(low, high, rounds, 0)

    def finish(m):
        def one(blk, carry):
            @pl.when(blk != f)
            def _():
                for o in range(1, nr):
                    y_arrival(m, blk, o).wait_recv()
            return carry

        lax.fori_loop(0, nf, one, 0)

    def drain(m):
        for way in (0, 1):
            for back in (0, 1):
                last = hops[way] - back

                @pl.when(jnp.logical_and(can_send[way], last >= 0))
                def _():
                    z_copy(m, f, way, last).wait_send()

                @pl.when(last >= 1)
                def _():
                    for o in range(1, nr):
                        y_copy(m, f, way, last, o).wait_send()

    def share_of(ref, j):
        return ref.at[pl.ds(pl.multiple_of(j * share, share), share), :]

    def normalize(load, gain, store, count):
        def square(i, total):
            v = load(i)
            return total + jnp.sum(v * v, axis=0, keepdims=True)

        total = lax.fori_loop(0, count, square, jnp.zeros((1, tokens), F32))
        factor = lax.rsqrt(total / features + EPS)

        def scaled(i, carry):
            store(i, load(i) * factor * column(gain[pl.ds(i, 1), :], tokens))
            return carry

        lax.fori_loop(0, count, scaled, 0)

    def chunk(ref, i):
        return ref[pl.ds(pl.multiple_of(i * LANES, LANES), LANES), :].astype(F32)

    def put(ref):
        def store(i, v):
            ref[pl.ds(pl.multiple_of(i * LANES, LANES), LANES), :] = v.astype(ref.dtype)
        return store

    def a_copy(k, part, c):
        return pltpu.make_async_remote_copy(
            src_ref=share_of(part, 2 * c + 1 - parity), dst_ref=buf_a.at[k, c],
            send_sem=a_send.at[k, c], recv_sem=a_recv.at[k, c],
            device_id=(r, f, partner), device_id_type=MESH,
        )

    def b_copy(k, part, i):
        target = 2 * lax.rem(chip + i, nh) + parity
        return pltpu.make_async_remote_copy(
            src_ref=share_of(part, target), dst_ref=buf_b.at[k, i],
            send_sem=b_send.at[k, i], recv_sem=b_recv.at[k, i],
            device_id=(r, f, target), device_id_type=MESH,
        )

    def start_pair(k, part):
        for i in range(nh):
            a_copy(k, part, i).start()

    def start_chips(k, part):
        for i in range(1, nh):
            c = lax.rem(chip + i, nh)
            target = 2 * c + parity
            a_copy(k, part, c).wait()

            def add(n, carry):
                at = pl.ds(pl.multiple_of(target * share + n * LANES, LANES), LANES)
                mine = part[at, :].astype(F32)
                theirs = buf_a[k, c, pl.ds(pl.multiple_of(n * LANES, LANES), LANES), :].astype(F32)
                part[at, :] = (mine + theirs).astype(BF)
                return carry

            lax.fori_loop(0, share // LANES, add, 0)
            b_copy(k, part, i).start()

    def finish_chips(k, part, base, store):
        a_copy(k, part, chip).wait()
        for i in range(1, nh):
            b_copy(k, part, i).wait()

        def add(n, carry):
            here = pl.ds(pl.multiple_of(n * LANES, LANES), LANES)
            at = pl.ds(pl.multiple_of(t * share + n * LANES, LANES), LANES)
            total = part[at, :].astype(F32) + buf_a[k, chip, here, :].astype(F32)
            for i in range(1, nh):
                total = total + buf_b[k, i, here, :].astype(F32)
            store(n, base[at, :].astype(F32) + total)
            return carry

        lax.fori_loop(0, share // LANES, add, 0)

    def c_copy(i):
        ref = share_of(x1, t)
        return pltpu.make_async_remote_copy(
            src_ref=ref, dst_ref=ref, send_sem=c_send.at[i], recv_sem=c_recv.at[i],
            device_id=(r, f, 2 * lax.rem(chip + i, nh) + parity), device_id_type=MESH,
        )

    def d_copy(i):
        ref = share_of(x1, 2 * lax.rem(chip - i + nh, nh) + parity)
        return pltpu.make_async_remote_copy(
            src_ref=ref, dst_ref=ref, send_sem=d_send.at[i], recv_sem=d_recv.at[i],
            device_id=(r, f, partner), device_id_type=MESH,
        )

    def s_copy(i):
        return pltpu.make_async_remote_copy(
            src_ref=squares.at[0], dst_ref=squares.at[i], send_sem=s_send.at[i], recv_sem=s_recv.at[i],
            device_id=(r, f, lax.rem(t + i, nt)), device_id_type=MESH,
        )

    send_own(0)
    normalize(functools.partial(chunk, act), g_mix, put(h), features // LANES)

    gather(0, 1, nf)
    gather(1, 1, nf)
    finish(0)
    u_acc[...] = jnp.zeros_like(u_acc)

    def mix_in(b, carry):
        at = pl.ds(pl.multiple_of(b * rows, rows), rows)
        u_acc[...] += dot_first(b_in[b], h[at, :])
        return carry

    lax.fori_loop(0, nf, mix_in, 0)
    for i in range(channels // LANES):
        first = t * channels + i * LANES
        window = jnp.int32(2) << (first // POOL_GROUP)
        behind = window // 2
        onward = window - behind
        source = lax.broadcasted_iota(jnp.int32, (SEQ_LEN, SEQ_LEN), 0)
        place = lax.broadcasted_iota(jnp.int32, (SEQ_LEN, SEQ_LEN), 1)
        inside = jnp.logical_and(source >= place - behind, source < place + onward)
        band = jnp.where(inside, 1.0, 0.0).astype(BF)
        spot = lax.broadcasted_iota(jnp.int32, (1, SEQ_LEN), 1)
        count = (jnp.minimum(spot + onward, SEQ_LEN) - jnp.maximum(spot - behind, 0)).astype(F32)
        gain = column(scale[pl.ds(first // LANES, 1), :], SEQ_LEN)
        for s in range(tokens // SEQ_LEN):
            at = (pl.ds(i * LANES, LANES), pl.ds(s * SEQ_LEN, SEQ_LEN))
            u = u_acc[at].astype(BF)
            mean = jnp.dot(u, band, preferred_element_type=F32) / count
            pooled[at] = ((mean - u.astype(F32)) * gain).astype(BF)

    gather(2, 1, nf)
    finish(1)

    def mix_out(b, carry):
        at = pl.ds(pl.multiple_of(b * rows, rows), rows)
        part0[at, :] = jnp.dot(b_out[b], pooled[...], preferred_element_type=F32).astype(BF)
        return carry

    lax.fori_loop(0, nf, mix_out, 0)
    start_pair(0, part0)
    gather(3, 1, nf)
    start_chips(0, part0)
    gather(4, 1, nf)

    def keep_x1(n, v):
        at = pl.ds(pl.multiple_of(t * share + n * LANES, LANES), LANES)
        x1[at, :] = v.astype(BF)

    finish_chips(0, part0, act, keep_x1)
    for i in range(1, nh):
        c_copy(i).start()
    d_copy(0).start()
    gather(5, 1, nf)
    for i in range(1, nh):
        c_copy(i).wait()
        d_copy(i).start()
    gather(6, 1, nf)
    for i in range(nh):
        d_copy(i).wait()
    normalize(functools.partial(chunk, x1), g_ffn, put(h), features // LANES)
    finish(2)
    finish(3)
    gate_acc[...] = jnp.zeros_like(gate_acc)
    up_acc[...] = jnp.zeros_like(up_acc)

    def project(source, acc):
        def one(b, carry):
            at = pl.ds(pl.multiple_of(b * rows, rows), rows)
            acc[...] += dot_first(source[b], h[at, :])
            return carry

        lax.fori_loop(0, nf, one, 0)

    gather(7, 1, nf)
    project(b_gate, gate_acc)
    finish(4)
    finish(5)
    project(b_up, up_acc)
    step = 32

    def activate(n, carry):
        at = pl.ds(pl.multiple_of(n * step, step), step)
        v = gate_acc[at, :]
        hidden[at, :] = (v / (1.0 + jnp.exp(-v)) * up_acc[at, :]).astype(BF)
        return carry

    lax.fori_loop(0, ff // step, activate, 0)
    finish(6)
    finish(7)

    def mlp_out(b, carry):
        at = pl.ds(pl.multiple_of(b * rows, rows), rows)
        part1[at, :] = jnp.dot(b_down[b], hidden[...], preferred_element_type=F32).astype(BF)
        return carry

    if share % rows == 0:
        blocks = share // rows

        def pair_out(c):
            theirs, ours = 2 * c + 1 - parity, 2 * c + parity
            lax.fori_loop(theirs * blocks, (theirs + 1) * blocks, mlp_out, 0)
            a_copy(1, part1, c).start()
            lax.fori_loop(ours * blocks, (ours + 1) * blocks, mlp_out, 0)

        for i in range(1, nh):
            pair_out(lax.rem(chip + i, nh))
        start_chips(1, part1)
        pair_out(chip)
    else:
        lax.fori_loop(0, nf, mlp_out, 0)
        start_pair(1, part1)
        start_chips(1, part1)
    for m in range(len(items)):
        drain(m)
    finish_chips(1, part1, x1, put(own_x))

    def square(i, total):
        v = chunk(own_x, i)
        return total + jnp.sum(v * v, axis=0, keepdims=True)

    mine = lax.fori_loop(0, share // LANES, square, jnp.zeros((1, tokens), F32))
    squares[0] = jnp.broadcast_to(mine, squares.shape[1:])
    for i in range(1, nt):
        s_copy(i).start()
    for i in range(1, nt):
        s_copy(i).wait()
    total = squares[0, pl.ds(0, 1), :]
    for i in range(1, nt):
        total = total + squares[i, pl.ds(0, 1), :]
    factor = lax.rsqrt(total / features + EPS)

    def closing(i, carry):
        gain = column(g_out[pl.ds(t * (share // LANES) + i, 1), :], tokens)
        put(out)(i, chunk(own_x, i) * factor * gain)
        return carry

    lax.fori_loop(0, share // LANES, closing, 0)


def staged(
    nr, nf, nt,
    act, w_in, w_out, w_gate, w_up, w_down, scale, g_mix, g_ffn, g_out, out,
    b_in, b_out, b_gate, b_up, b_down,
    x0, h, x1, part, pooled, gate_acc, up_acc, hidden, own_x, squares, power,
    buf_a, buf_b, back, home,
    own_sem, act_sem, in_send, out_send, zrecv, wrecv, ysend, yrecv, v_send, v_recv,
    a_send, a_recv, b_send, b_recv, c_send, c_recv, d_send, d_recv,
    e_send, e_recv, g_send, g_recv, s_send, s_recv,
):
    r, f, t = lax.axis_index("rep"), lax.axis_index("fs"), lax.axis_index("tp")
    features, tokens = act.shape
    shards = (w_in, w_out, w_gate, w_up, w_down)
    full = (b_in, b_out, b_gate, b_up, b_down)
    rows, channels = w_in.shape
    ff = w_gate.shape[0]
    share = features // nt
    nh = nt // 2
    nq = share // LANES
    chip, parity = t // 2, lax.rem(t, 2)
    partner = t + 1 - 2 * parity
    other_rep = lax.rem(r + 1, nr)
    cuts = 2
    slab = share // cuts
    items = [(0, 0), (0, 1), (1, 0), (1, 1), (2, 0), (3, 0), (2, 1), (3, 1), (4, 0), (4, 1)]
    early = 4
    extra = 7
    last = len(items)
    left = f < nf // 2
    inner = jnp.logical_and(f >= 1, f < nf - 1)
    outer = jnp.logical_not(inner)
    mate = jnp.where(left, 1 - f, 2 * nf - 3 - f)
    inward = jnp.where(left, f + 1, f - 1)
    over = jnp.where(inner, nf - 1 - f, nf - 1 - mate)
    far = jnp.where(inner, nf - 1 - mate, nf - 1 - f)
    blocks = (mate, over, far)

    own = [pltpu.make_async_copy(shards[m], full[m].at[f], own_sem.at[m]) for m in range(5)]
    stream = [pltpu.make_async_copy(act, x0, act_sem.at[0])]
    own[0].start()
    own[1].start()
    for copy in stream:
        copy.start()
    for copy in own[2:]:
        copy.start()

    barrier = pltpu.get_barrier_semaphore()
    for step in (1, nf - 1):
        pl.semaphore_signal(barrier, inc=1, device_id=(r, lax.rem(f + step, nf), t), device_id_type=MESH)
    pl.semaphore_signal(barrier, inc=1, device_id=(other_rep, f, t), device_id_type=MESH)
    for i in range(1, nt):
        pl.semaphore_signal(barrier, inc=1, device_id=(r, f, lax.rem(t + i, nt)), device_id_type=MESH)
    pl.semaphore_wait(barrier, 3 + (nt - 1))

    def line(start, size=LANES):
        return pl.ds(pl.multiple_of(start, size), size)

    def part_of(m, blk, of):
        matrix, s = items[m]
        if matrix < 2:
            size = rows // cuts // nr
            return full[matrix].at[blk, line((s * nr + of) * size, size), :]
        if matrix < 4:
            size = ff // cuts // nr
            return full[matrix].at[blk, line((s * nr + of) * size, size), :]
        size = rows // cuts // nr
        return full[matrix].at[blk, :, line((s * nr + of) * size, size)]

    def remote(ref, dst, send, recv, device):
        return pltpu.make_async_remote_copy(
            src_ref=ref, dst_ref=dst, send_sem=send, recv_sem=recv, device_id=device, device_id_type=MESH
        )

    def group(m):
        return max(items[m][0] - 1, 0)

    def in_copy(m, blk, d):
        ref = part_of(m, blk, r)
        place = jnp.where(inner, 1, 0) if d == 0 else 2
        return remote(ref, ref, in_send.at[group(m)], zrecv.at[m, place], (r, inward, t))

    def out_copy(m, blk, j):
        ref = part_of(m, blk, r)
        return remote(ref, ref, out_send.at[0], zrecv.at[m, j], (r, mate, t))

    def arrive(m, j):
        ref = part_of(m, blocks[j], r)
        remote(ref, ref, in_send.at[group(m)], zrecv.at[m, j], (r, mate, t)).wait_recv()

    def lot(m):
        return (m - early) // 2 if m < 2 * cuts + early else m - early - cuts

    def w_copy(m, blk):
        ref = part_of(m, blk, other_rep)
        return remote(ref, ref, in_send.at[group(m)], wrecv.at[lot(m)], (r, mate, t))

    def v_copy(blk):
        ref = part_of(extra, blk, other_rep)
        return remote(ref, ref, v_send.at[0], v_recv.at[0], (r, inward, t))

    def y_copy(m, j, of):
        ref = part_of(m, blocks[j], of)
        place = m // 2 if m < last - 2 else last // 2 + 2 * (m - last + 2) + j - 2
        if items[m][0] == 1 and j == 0:
            place = last - 2
        return remote(ref, ref, ysend.at[group(m)], yrecv.at[place], (other_rep, f, t))

    def y_lot(ref, place):
        return remote(ref, ref, ysend.at[0], yrecv.at[place], (other_rep, f, t))

    def own_ready(m):
        if items[m][1] == 0:
            own[items[m][0]].wait()

    def send_mixer(m):
        own_ready(m)
        in_copy(m, f, 0).start()

        @pl.when(inner)
        def _():
            out_copy(m, f, 0).start()

    def hop(m, j):
        arrive(m, j)
        if j == 0:
            in_copy(m, mate, 1).start()
        else:
            out_copy(m, blocks[j], j).start()

    def side(m, j):
        y_copy(m, j, r).start()

    def relay(m, j):
        hop(m, j)
        side(m, j)

    def collect(m, j):
        arrive(m, j)
        side(m, j)

    def y_arrival(m, j):
        y_copy(m, j, other_rep).wait_recv()

    def finish(matrix, count, place):
        y_lot(full[matrix].at[pl.ds(0, count), pl.ds(0, rows // nr)], place).wait_recv()

    def send_inner(m):
        in_copy(m, f, 0).start()

    def send_outer(m):
        in_copy(m, f, 0).start()
        w_copy(m, f).start()

    def pass_on(m):
        hop(m, 0)

    def cross(m, *some):
        for j in some:
            arrive(m, j)
            if m != extra or j == 2:
                side(m, j)

    def settle(s):
        ref = full[2].at[0, pl.ds(0, ff // cuts)]
        remote(ref, ref, in_send.at[1], wrecv.at[s], (r, mate, t)).wait_recv()
        pieces = 2 * nr - (s == cuts - 1)
        y_lot(full[2].at[0, pl.ds(0, pieces * (ff // cuts // nr))], 2 + s).wait_recv()
        if s == cuts - 1:
            v_copy(over).wait_recv()

    def spot(target, q, size=LANES):
        return line(target * share + q * size, size)

    def normalize(load, gain, store, count):
        def square(i, total):
            v = load(i)
            return total + jnp.sum(v * v, axis=0, keepdims=True)

        total = lax.fori_loop(0, count, square, jnp.zeros((1, tokens), F32))
        factor = lax.rsqrt(total / features + EPS)

        def scaled(i, carry):
            store(i, load(i) * factor * column(gain[pl.ds(i, 1), :], tokens))
            return carry

        lax.fori_loop(0, count, scaled, 0)

    def chunk(ref, i):
        return ref[line(i * LANES), :].astype(F32)

    def put(ref):
        def store(i, v):
            ref[line(i * LANES), :] = v.astype(ref.dtype)
        return store

    def a_copy(k, target, q, size):
        return remote(
            part.at[k, spot(target, q, size)], buf_a.at[k, target // 2, line(q * size, size)],
            a_send.at[k], a_recv.at[k, target // 2, q], (r, f, partner),
        )

    def b_copy(k, i, q, size):
        target = 2 * lax.rem(chip + i, nh) + parity
        return remote(
            part.at[k, spot(target, q, size)], buf_b.at[k, i, line(q * size, size)],
            b_send.at[k], b_recv.at[k, i - 1, q], (r, f, target),
        )

    def c_copy(k, i, q):
        ref = x1.at[k, spot(t, q)]
        device = (r, f, 2 * lax.rem(chip + i, nh) + parity)
        return remote(ref, ref, c_send.at[k], c_recv.at[k, i - 1, q], device)

    def d_copy(k, i, q):
        ref = x1.at[k, spot(2 * lax.rem(chip - i + nh, nh) + parity, q)]
        return remote(ref, ref, d_send.at[k], d_recv.at[k, i], (r, f, partner))

    def e_copy(q):
        return remote(x1.at[0, spot(t, q)], x1.at[1, spot(t, q)], e_send.at[0], e_recv.at[q], (r, mate, t))

    def g_copy(q):
        return remote(back.at[line(q * LANES)], home.at[line(q * LANES)], g_send.at[0], g_recv.at[q], (r, mate, t))

    def s_copy(i):
        return remote(squares.at[0], squares.at[i], s_send.at[0], s_recv.at[0], (r, f, lax.rem(t + i, nt)))

    def add_pair(k, target, q, size):
        for n in range(size // LANES):
            here = line(q * size + n * LANES)
            at = line(target * share + q * size + n * LANES)
            mine, theirs = part[k, at, :].astype(F32), buf_a[k, target // 2, here, :].astype(F32)
            part[k, at, :] = (mine + theirs).astype(BF)

    def total_of(k, q):
        here = line(q * LANES)
        total = part[k, spot(t, q), :].astype(F32) + buf_a[k, chip, here, :].astype(F32)
        for i in range(1, nh):
            total = total + buf_b[k, i, here, :].astype(F32)
        return total

    send_mixer(0)
    send_mixer(1)
    for m in (2, 4, 5, 8):
        own_ready(m)

    @pl.when(outer)
    def _():
        for m in (2, 3):
            in_copy(m, f, 0).start()
        for m in (4, 5, 6):
            send_outer(m)
        send_outer(7)

    @pl.when(inner)
    def _():
        in_copy(2, f, 0).start()

    for copy in stream:
        copy.wait()
    normalize(functools.partial(chunk, x0), g_mix, put(h.at[0]), features // LANES)

    @pl.when(inner)
    def _():
        relay(0, 0)
        relay(0, 1)
        relay(1, 0)
        relay(1, 1)
        in_copy(3, f, 0).start()
        hop(2, 0)
        hop(3, 0)
        send_inner(4)
        relay(0, 2)
        relay(1, 2)
        relay(2, 1)
        relay(3, 1)
        pass_on(4)
        send_inner(5)

    @pl.when(outer)
    def _():
        for j in range(3):
            collect(0, j)
            collect(1, j)

    finish(0, nf - 1, 0)

    u_mix = dot_first(b_in[0], h[0, pl.ds(0, rows), :])
    for b in range(1, nf):
        u_mix += dot_first(b_in[b], h[0, pl.ds(b * rows, rows), :])
    gate_acc[pl.ds(0, channels), :] = u_mix
    for i in range(channels // LANES):
        first = t * channels + i * LANES
        window = jnp.int32(2) << (first // POOL_GROUP)
        behind = window // 2
        onward = window - behind
        source = lax.broadcasted_iota(jnp.int32, (SEQ_LEN, SEQ_LEN), 0)
        place = lax.broadcasted_iota(jnp.int32, (SEQ_LEN, SEQ_LEN), 1)
        inside = jnp.logical_and(source >= place - behind, source < place + onward)
        band = jnp.where(inside, 1.0, 0.0).astype(BF)
        seat = lax.broadcasted_iota(jnp.int32, (1, SEQ_LEN), 1)
        count = (jnp.minimum(seat + onward, SEQ_LEN) - jnp.maximum(seat - behind, 0)).astype(F32)
        gain = column(scale[pl.ds(first // LANES, 1), :], SEQ_LEN)
        for s in range(tokens // SEQ_LEN):
            at = (pl.ds(i * LANES, LANES), pl.ds(s * SEQ_LEN, SEQ_LEN))
            u = gate_acc[at].astype(BF)
            mean = jnp.dot(u, band, preferred_element_type=F32) / count
            pooled[at] = ((mean - u.astype(F32)) * gain).astype(BF)

    mixed = True

    def mix_out(target):
        part[0, line(target * share, share), :] = jnp.dot(
            b_out[target], pooled[...], preferred_element_type=F32
        ).astype(BF)

        @pl.when(lax.rem(target, 2) != parity)
        def _():
            a_copy(0, target, 0, share).start()

    def reduce_pair(target):
        @pl.when(lax.rem(target, 2) == parity)
        def _():
            a_copy(0, target, 0, share).wait_recv()
            for i in range(1, nh):
                @pl.when(target // 2 == lax.rem(chip + i, nh))
                def _():
                    for q in range(nq):
                        add_pair(0, target, q, LANES)
                        b_copy(0, i, q, LANES).start()

    mix_out(f)

    @pl.when(inner)
    def _():
        relay(2, 2)
        relay(3, 2)
        side(2, 0)
        side(3, 0)
        for m in (2, 3):
            out_copy(m, f, 0).start()

    reduce_pair(f)

    @pl.when(inner)
    def _():
        cross(4, 1)
        pass_on(5)
        send_inner(6)

    @pl.when(outer)
    def _():
        for j in (1, 2):
            collect(2, j)
            collect(3, j)
        collect(2, 0)
        collect(3, 0)

    finish(1, 2, 1)
    mix_out(over)
    mix_out(far)
    reduce_pair(over)
    reduce_pair(far)

    @pl.when(inner)
    def _():
        cross(4, 2)

    finish(1, 1, last - 2)
    mix_out(mate)
    reduce_pair(mate)

    @pl.when(inner)
    def _():
        cross(5, 1)

    def prepare(k, target, q):
        at = spot(target, q)
        v = x1[k, at, :].astype(F32)
        h[k, at, :] = (v * column(g_ffn[pl.ds(target * nq + q, 1), :], tokens)).astype(BF)
        power[k] += jnp.sum((v * v).reshape(LANES // 8, 8, tokens), axis=0)

    power[...] = jnp.zeros_like(power)

    for q in range(nq):
        for i in range(1, nh):
            b_copy(0, i, q, LANES).wait_recv()
        x1[0, spot(t, q), :] = (x0[spot(t, q), :].astype(F32) + total_of(0, q)).astype(BF)

        @pl.when(inner)
        def _():
            for i in range(1, nh):
                c_copy(0, i, q).start()
            d_copy(0, 0, q).start()
            prepare(0, t, q)
            if q == 0:
                pass_on(6)
                send_inner(7)
                cross(5, 2)
            if q == 1:
                cross(6, 1)
            if q == 2:
                pass_on(7)
                v_copy(f).start()
                send_inner(8)
                send_inner(9)

        @pl.when(outer)
        def _():
            e_copy(q).start()

    cut = ff // cuts
    step = 32
    wide = 2 * LANES

    def project(k, s, targets, fresh):
        at = pl.ds(s * cut, cut)
        for source, acc in ((b_gate, gate_acc), (b_up, up_acc)):
            def tokens_at(n, carry):
                here = line(n * wide, wide)
                terms = [
                    jnp.dot(source[b, at, :], h[k, line(b * rows, rows), here], preferred_element_type=F32)
                    for b in targets
                ]
                total = functools.reduce(lambda x, y: x + y, terms)
                acc[at, here] = total if fresh else acc[at, here] + total
                return carry

            lax.fori_loop(0, tokens // wide, tokens_at, 0)

    def activate(k, s):
        total = jnp.sum(power[k], axis=0, keepdims=True)
        factor = lax.rsqrt(total / features + EPS)

        def some(n, carry):
            here = line(s * cut + n * step, step)
            v = gate_acc[here, :] * factor
            hidden[k, here, :] = (v / (1.0 + jnp.exp(-v)) * (up_acc[here, :] * factor)).astype(BF)
            return carry

        lax.fori_loop(0, cut // step, some, 0)

    def mlp_out(k, target, s):
        at = spot(target, s, slab)
        part[1 + k, at, :] = dot_first(b_down[target, :, line(s * slab, slab)], hidden[k]).astype(BF)

        @pl.when(lax.rem(target, 2) != parity)
        def _():
            a_copy(1 + k, target, s, slab).start()

    def pair_up(k, target, s):
        @pl.when(lax.rem(target, 2) == parity)
        def _():
            a_copy(1 + k, target, s, slab).wait_recv()
            for i in range(1, nh):
                @pl.when(target // 2 == lax.rem(chip + i, nh))
                def _():
                    add_pair(1 + k, target, s, slab)
                    b_copy(1 + k, i, s, slab).start()

    plans = (
        [(1, 2, 0), (1, 2, 1), (1, 0, 0), (1, 0, 1), (1, 3, 0), (1, 1, 0), (1, 3, 1), (1, 1, 1),
         (0, 2, 1), (0, 3, 0), (0, 3, 1), (0, 0, 0), (0, 0, 1), (0, 1, 0), (0, 1, 1)],
        [(1, 0, 0), (1, 0, 1), (1, 1, 0), (1, 2, 0), (1, 2, 1), (1, 1, 1), (1, 3, 0), (1, 3, 1),
         (0, 0, 1), (0, 1, 0), (0, 1, 1), (0, 2, 0), (0, 3, 0), (0, 2, 1), (0, 3, 1)],
    )
    soon = jnp.logical_or(t == f, t == over)
    near = chip == f // 2

    def planned(n):
        k, s, target = jnp.int32(0), jnp.int32(0), f
        for plan, taken in zip(plans, (near, jnp.logical_not(near))):
            for at, (kk, code, ss) in enumerate(plan):
                here = jnp.logical_and(n == at, taken)
                k = jnp.where(here, kk, k)
                s = jnp.where(here, ss, s)
                target = jnp.where(here, (f, mate, over, far)[code], target)
        return k, target, s

    def give_back(s):
        for i in range(1, nh):
            b_copy(2, i, s, slab).wait_recv()
        for n in range(slab // LANES):
            q = s * (slab // LANES) + n
            back[pl.ds(q * LANES, LANES), :] = total_of(2, q).astype(BF)
            g_copy(q).start()

    def spread(q):
        e_copy(q).wait_recv()
        for i in range(1, nh):
            c_copy(1, i, q).start()
        d_copy(1, 0, q).start()
        prepare(1, t, q)

    def mine(i):
        return 2 * lax.rem(chip - i + nh, nh) + parity

    def theirs(i):
        return 2 * lax.rem(chip - i + nh, nh) + 1 - parity

    def hand_over(k, q):
        for i in range(1, nh):
            c_copy(k, i, q).wait_recv()
            d_copy(k, i, q).start()
            prepare(k, mine(i), q)

    def absorb(k, i):
        ref = x1.at[k, line(theirs(i) * share, share)]
        remote(ref, ref, d_send.at[k], d_recv.at[k, i], (r, f, partner)).wait_recv()
        for q in range(nq):
            prepare(k, theirs(i), q)

    here_blocks = (t, partner)
    away_blocks = tuple(b for i in range(1, nh) for b in (mine(i), theirs(i)))

    @pl.when(inner)
    def _():
        cross(6, 2)
        absorb(0, 0)
        hand_over(0, 0)
        settle(0)
        project(0, 0, here_blocks, True)
        cross(7, 1)
        hand_over(0, 1)
        spread(0)
        cross(7, 2)
        hand_over(0, 2)
        spread(1)
        hand_over(0, 3)
        spread(2)
        for i in range(1, nh):
            absorb(0, i)
        project(0, 0, away_blocks, False)
        activate(0, 0)
        spread(3)
        hand_over(1, 0)
        absorb(1, 0)
        project(1, 0, here_blocks, True)
        cross(8, 1)
        pass_on(8)
        hand_over(1, 1)
        settle(1)
        project(0, 1, here_blocks + away_blocks, True)
        activate(0, 1)
        hand_over(1, 2)
        pass_on(9)
        project(1, 1, here_blocks, True)
        cross(9, 1)

        @pl.when(near)
        def _():
            y_arrival(8, 1)

        lead = jnp.where(near, over, f)
        mlp_out(0, lead, 0)
        hand_over(1, 3)
        for i in range(1, nh):
            absorb(1, i)
        cross(8, 2)
        pair_up(0, lead, 0)
        project(1, 0, away_blocks, False)
        activate(1, 0)
        project(1, 1, away_blocks, False)
        cross(9, 2)
        activate(1, 1)

        def ffn(n, carry):
            near_waits = (
                (1, lambda: y_arrival(9, 1)),
                (4, lambda: y_arrival(8, 2)),
                (5, lambda: w_copy(8, mate).wait_recv()),
                (6, lambda: y_arrival(9, 2)),
                (7, lambda: w_copy(9, mate).wait_recv()),
            )
            away_waits = (
                (2, lambda: w_copy(8, mate).wait_recv()),
                (3, lambda: y_arrival(8, 1)),
                (4, lambda: y_arrival(9, 1)),
                (5, lambda: w_copy(9, mate).wait_recv()),
                (6, lambda: y_arrival(8, 2)),
                (7, lambda: y_arrival(9, 2)),
            )
            for waits, taken in ((near_waits, near), (away_waits, jnp.logical_not(near))):
                for at, wait in waits:
                    @pl.when(jnp.logical_and(n == at, taken))
                    def _():
                        wait()

            for s, first, second in ((0, 8, 10), (1, 9, 13)):
                @pl.when(n == jnp.where(soon, first, second))
                def _():
                    give_back(s)

            mlp_out(*planned(n))

            @pl.when(n >= 1)
            def _():
                pair_up(*planned(n - 1))
            return carry

        lax.fori_loop(0, len(plans[0]), ffn, 0)
        pair_up(*planned(len(plans[0]) - 1))
        for q in range(nq):
            for i in range(1, nh):
                if q % (slab // LANES) == 0:
                    b_copy(1, i, q // (slab // LANES), slab).wait_recv()
            own_x[pl.ds(q * LANES, LANES), :] = x1[0, spot(t, q), :].astype(F32) + total_of(1, q)

    @pl.when(outer)
    def _():
        for m in (8, 9):
            in_copy(m, f, 0).start()
        for m in (8, 9):
            w_copy(m, f).start()
        for q in range(nq):
            g_copy(q).wait_recv()
            at = pl.ds(q * LANES, LANES)
            own_x[at, :] = x1[0, spot(t, q), :].astype(F32) + home[at, :].astype(F32)

    total = jnp.zeros((1, tokens), F32)
    for q in range(nq):
        v = own_x[pl.ds(q * LANES, LANES), :]
        total += jnp.sum(v * v, axis=0, keepdims=True)
    squares[0] = jnp.broadcast_to(total, squares.shape[1:])
    for i in range(1, nt):
        s_copy(i).start()

    got = squares.at[pl.ds(1, nt - 1)]
    remote(got, got, s_send.at[0], s_recv.at[0], (r, f, partner)).wait_recv()
    for i in range(1, nt):
        total = total + squares[i, pl.ds(0, 1), :]
    factor = lax.rsqrt(total / features + EPS)

    def closing(q):
        gain = column(g_out[pl.ds(t * nq + q, 1), :], tokens)
        out[pl.ds(q * LANES, LANES), :] = (own_x[pl.ds(q * LANES, LANES), :] * factor * gain).astype(BF)

    for q in range(nq):
        closing(q)

    def sent(ref, sem):
        remote(ref, ref, sem, zrecv.at[0, 0], (r, mate, t)).wait_send()

    for matrix in (2, 3, 4):
        sent(full[matrix].at[0], in_send.at[matrix - 1])
    sent(full[0].at[pl.ds(0, nf - 1)], ysend.at[0])
    sent(part.at[0, pl.ds(0, nh * share)], a_send.at[0])
    sent(part.at[0, pl.ds(0, (nh - 1) * share)], b_send.at[0])
    sent(squares.at[pl.ds(1, nt - 1)], s_send.at[0])

    @pl.when(inner)
    def _():
        sent(full[0].at[pl.ds(0, 2)], in_send.at[0])
        sent(full[0].at[pl.ds(0, nf - 1)], out_send.at[0])
        v_copy(f).wait_send()
        sent(full[2].at[0], ysend.at[1])
        sent(full[3].at[0, pl.ds(0, (2 * nr - 1) * (ff // cuts // nr))], ysend.at[2])
        sent(full[4].at[0], ysend.at[3])
        for k in (0, 1):
            sent(part.at[0, pl.ds(0, nh * share)], a_send.at[1 + k])
            sent(part.at[0, pl.ds(0, (nh - 1) * share)], b_send.at[1 + k])
            sent(part.at[0, pl.ds(0, nh * share)], d_send.at[k])
            sent(part.at[0, pl.ds(0, (nh - 1) * share)], c_send.at[k])
        sent(back, g_send.at[0])

    @pl.when(outer)
    def _():
        sent(full[0].at[0], in_send.at[0])
        sent(back, e_send.at[0])


def solution(mesh):
    nr, nf, nt = mesh.shape["rep"], mesh.shape["fs"], mesh.shape["tp"]

    def staged_call(act, w_in, w_out, w_gate, w_up, w_down, scale, g_mix, g_ffn, g_out):
        features, tokens = act.shape
        rows, channels = w_in.shape
        ff = w_gate.shape[1]
        share = features // nt
        nh = nt // 2
        nq = share // LANES
        anywhere = pl.BlockSpec(memory_space=pl.ANY)
        vmem = pl.BlockSpec(memory_space=pltpu.VMEM)
        dma = pltpu.SemaphoreType.DMA
        scratch = [
            pltpu.VMEM((nf, rows, channels), BF),
            pltpu.VMEM((nf, rows, channels), BF),
            pltpu.VMEM((nf, ff, rows), BF),
            pltpu.VMEM((nf, ff, rows), BF),
            pltpu.VMEM((nf, ff, rows), BF),
            pltpu.VMEM((features, tokens), BF),
            pltpu.VMEM((2, features, tokens), BF),
            pltpu.VMEM((2, features, tokens), BF),
            pltpu.VMEM((3, features, tokens), BF),
            pltpu.VMEM((channels, tokens), BF),
            pltpu.VMEM((ff, tokens), F32),
            pltpu.VMEM((ff, tokens), F32),
            pltpu.VMEM((2, ff, tokens), BF),
            pltpu.VMEM((share, tokens), F32),
            pltpu.VMEM((nt, 8, tokens), F32),
            pltpu.VMEM((2, 8, tokens), F32),
            pltpu.VMEM((3, nh, share, tokens), BF),
            pltpu.VMEM((3, nh, share, tokens), BF),
            pltpu.VMEM((share, tokens), BF),
            pltpu.VMEM((share, tokens), BF),
            dma((5,)), dma((1,)),
            dma((4,)), dma((1,)), dma((10, 3)), dma((4,)), dma((4,)), dma((9,)), dma((1,)), dma((1,)),
            dma((3,)), dma((3, nh, 2)), dma((3,)), dma((3, nh - 1, nq)),
            dma((2,)), dma((2, nh - 1, nq)), dma((2,)), dma((2, nh)),
            dma((1,)), dma((nq,)), dma((1,)), dma((nq,)), dma((1,)), dma((1,)),
        ]
        return pl.pallas_call(
            functools.partial(staged, nr, nf, nt),
            out_shape=jax.ShapeDtypeStruct((share, tokens), BF),
            in_specs=[anywhere] * 6 + [vmem] * 4,
            out_specs=vmem,
            scratch_shapes=scratch,
            compiler_params=pltpu.CompilerParams(
                collective_id=0, has_side_effects=True, vmem_limit_bytes=60 * 1024 * 1024
            ),
        )(
            act, w_in, w_out, w_gate.T, w_up.T, w_down.T,
            *[v.reshape(-1, LANES) for v in (scale, g_mix, g_ffn, g_out)],
        )

    def on_device(act, w_in, w_out, w_gate, w_up, w_down, scale, g_mix, g_ffn, g_out):
        features, tokens = act.shape
        rows, channels = w_in.shape
        ff = w_gate.shape[1]
        share = features // nt
        nh = nt // 2
        if nr == 2 and nf == 4 and share == rows and rows % (2 * nr * LANES) == 0 and ff % (32 * nr) == 0:
            return staged_call(act, w_in, w_out, w_gate, w_up, w_down, scale, g_mix, g_ffn, g_out)
        anywhere = pl.BlockSpec(memory_space=pl.ANY)
        vmem = pl.BlockSpec(memory_space=pltpu.VMEM)
        dma = pltpu.SemaphoreType.DMA
        scratch = [
            pltpu.VMEM((nf, rows, channels), BF),
            pltpu.VMEM((nf, rows, channels), BF),
            pltpu.VMEM((nf, rows, ff), BF),
            pltpu.VMEM((nf, rows, ff), BF),
            pltpu.VMEM((nf, rows, ff), BF),
            pltpu.VMEM((features, tokens), BF),
            pltpu.VMEM((features, tokens), BF),
            pltpu.VMEM((features, tokens), BF),
            pltpu.VMEM((features, tokens), BF),
            pltpu.VMEM((channels, tokens), F32),
            pltpu.VMEM((channels, tokens), BF),
            pltpu.VMEM((ff, tokens), F32),
            pltpu.VMEM((ff, tokens), F32),
            pltpu.VMEM((ff, tokens), BF),
            pltpu.VMEM((share, tokens), F32),
            pltpu.VMEM((nt, 8, tokens), F32),
            pltpu.VMEM((2, nh, share, tokens), BF),
            pltpu.VMEM((2, nh, share, tokens), BF),
            dma((5,)),
            dma((8, 2, 2)),
            dma((8, nf)),
            dma((8, 2, 2, max(nr - 1, 1))),
            dma((8, nf, max(nr - 1, 1))),
            dma((2, nh)), dma((2, nh)), dma((2, nh)), dma((2, nh)),
            dma((nh,)), dma((nh,)), dma((nh,)), dma((nh,)),
            dma((nt,)), dma((nt,)),
        ]
        return pl.pallas_call(
            functools.partial(body, nr, nf, nt),
            out_shape=jax.ShapeDtypeStruct((share, tokens), BF),
            in_specs=[vmem] + [anywhere] * 5 + [vmem] * 4,
            out_specs=vmem,
            scratch_shapes=scratch,
            compiler_params=pltpu.CompilerParams(
                collective_id=0, has_side_effects=True, vmem_limit_bytes=60 * 1024 * 1024
            ),
        )(
            act, w_in, w_out, w_gate, w_up, w_down,
            *[v.reshape(-1, LANES) for v in (scale, g_mix, g_ffn, g_out)],
        )

    weight = P("fs", "tp")
    tokens_split = P(None, ("rep", "fs"))
    return jax.shard_map(
        on_device,
        mesh=mesh,
        in_specs=(tokens_split, *[weight] * 5, P(), P(), P(), P()),
        out_specs=P("tp", ("rep", "fs")),
        check_vma=False,
    )
```

```python
import functools

import jax
import jax.numpy as jnp
from jax import lax
from jax.experimental import pallas as pl
from jax.experimental.pallas import tpu as pltpu
from jax.sharding import PartitionSpec as P

POOL_GROUP = 256
SEQ_LEN = 256
EPS = 1e-06
LANES = 128
MESH = pl.DeviceIdType.MESH
BF = jnp.bfloat16
F32 = jnp.float32


def dot_first(weights, acts):
    return lax.dot_general(weights, acts, (((0,), (0,)), ((), ())), preferred_element_type=F32)


def column(row, width):
    square = jnp.transpose(jnp.broadcast_to(row, (LANES, LANES)))
    return jnp.concatenate([square] * (width // LANES), axis=1)


def body(
    nr, nf, nt,
    act, w_in, w_out, w_gate, w_up, w_down, scale, g_mix, g_ffn, g_out, out,
    b_in, b_out, b_gate, b_up, b_down,
    h, x1, part0, part1, u_acc, pooled, gate_acc, up_acc, hidden, own_x, squares,
    buf_a, buf_b,
    own_sem, zsend, zrecv, ysend, yrecv,
    a_send, a_recv, b_send, b_recv, c_send, c_recv, d_send, d_recv, s_send, s_recv,
):
    r, f, t = lax.axis_index("rep"), lax.axis_index("fs"), lax.axis_index("tp")
    features, tokens = act.shape
    shards = (w_in, w_out, w_gate, w_up, w_down)
    full = (b_in, b_out, b_gate, b_up, b_down)
    rows = w_in.shape[0]
    piece = rows // nr
    share = features // nt
    channels = w_in.shape[1]
    ff = w_gate.shape[1]
    nh = nt // 2
    chip, parity = t // 2, lax.rem(t, 2)
    partner = t + 1 - 2 * parity

    cut = -(-ff // (2 * LANES)) * LANES
    items = [(0, 0, channels), (1, 0, channels)]
    for m in (2, 3, 4):
        items += [(m, 0, cut), (m, cut, ff - cut)]

    own = [pltpu.make_async_copy(shards[m], full[m].at[f], own_sem.at[m]) for m in range(5)]
    for copy in own:
        copy.start()

    barrier = pltpu.get_barrier_semaphore()
    for step in (1, nf - 1):
        pl.semaphore_signal(barrier, inc=1, device_id=(r, lax.rem(f + step, nf), t), device_id_type=MESH)
    for o in range(1, nr):
        pl.semaphore_signal(barrier, inc=1, device_id=(lax.rem(r + o, nr), f, t), device_id_type=MESH)
    for i in range(1, nt):
        pl.semaphore_signal(barrier, inc=1, device_id=(r, f, lax.rem(t + i, nt)), device_id_type=MESH)
    pl.semaphore_wait(barrier, 2 + (nr - 1) + (nt - 1))

    def part_of(m, blk, of):
        matrix, start, size = items[m]
        at = pl.ds(pl.multiple_of(of * piece, piece), piece)
        return full[matrix].at[blk, at, pl.ds(start, size)]

    def z_copy(m, blk, way, d):
        ref = part_of(m, blk, r)
        return pltpu.make_async_remote_copy(
            src_ref=ref, dst_ref=ref,
            send_sem=zsend.at[m, way, lax.rem(d, 2)], recv_sem=zrecv.at[m, blk],
            device_id=(r, f + 1 - 2 * way, t), device_id_type=MESH,
        )

    def y_copy(m, blk, way, d, o):
        ref = part_of(m, blk, r)
        return pltpu.make_async_remote_copy(
            src_ref=ref, dst_ref=ref,
            send_sem=ysend.at[m, way, lax.rem(d, 2), o - 1], recv_sem=yrecv.at[m, blk, o - 1],
            device_id=(lax.rem(r + o, nr), f, t), device_id_type=MESH,
        )

    def y_arrival(m, blk, o):
        source = lax.rem(r - o + nr, nr)
        ref = part_of(m, blk, source)
        return pltpu.make_async_remote_copy(
            src_ref=ref, dst_ref=ref,
            send_sem=ysend.at[m, 0, 0, o - 1], recv_sem=yrecv.at[m, blk, o - 1],
            device_id=(lax.rem(r + o, nr), f, t), device_id_type=MESH,
        )

    can_send = (f + 1 < nf, f >= 1)
    hops = (f, nf - 1 - f)

    def send_own(m):
        if items[m][1] == 0:
            own[items[m][0]].wait()
        for way in (0, 1):
            @pl.when(can_send[way])
            def _():
                z_copy(m, f, way, 0).start()

    def arrival(m, way, d):
        blk = f - d if way == 0 else f + d

        @pl.when(d <= hops[way])
        def _():
            z_copy(m, blk, way, d).wait_recv()

            @pl.when(can_send[way])
            def _():
                @pl.when(d >= 2)
                def _():
                    z_copy(m, blk, way, d).wait_send()

                z_copy(m, blk, way, d).start()

            for o in range(1, nr):
                @pl.when(d >= 3)
                def _():
                    y_copy(m, blk, way, d, o).wait_send()

                y_copy(m, blk, way, d, o).start()

    def gather(m, low, high):
        if low >= high:
            return

        def rounds(d, carry):
            arrival(m, 0, d)
            arrival(m, 1, d)
            return carry

        if low == 1:
            rounds(jnp.int32(1), 0)
            if m + 1 < len(items):
                send_own(m + 1)
            low = 2
        lax.fori_loop(low, high, rounds, 0)

    def finish(m):
        def one(blk, carry):
            @pl.when(blk != f)
            def _():
                for o in range(1, nr):
                    y_arrival(m, blk, o).wait_recv()
            return carry

        lax.fori_loop(0, nf, one, 0)

    def drain(m):
        for way in (0, 1):
            for back in (0, 1):
                last = hops[way] - back

                @pl.when(jnp.logical_and(can_send[way], last >= 0))
                def _():
                    z_copy(m, f, way, last).wait_send()

                @pl.when(last >= 1)
                def _():
                    for o in range(1, nr):
                        y_copy(m, f, way, last, o).wait_send()

    def share_of(ref, j):
        return ref.at[pl.ds(pl.multiple_of(j * share, share), share), :]

    def normalize(load, gain, store, count):
        def square(i, total):
            v = load(i)
            return total + jnp.sum(v * v, axis=0, keepdims=True)

        total = lax.fori_loop(0, count, square, jnp.zeros((1, tokens), F32))
        factor = lax.rsqrt(total / features + EPS)

        def scaled(i, carry):
            store(i, load(i) * factor * column(gain[pl.ds(i, 1), :], tokens))
            return carry

        lax.fori_loop(0, count, scaled, 0)

    def chunk(ref, i):
        return ref[pl.ds(pl.multiple_of(i * LANES, LANES), LANES), :].astype(F32)

    def put(ref):
        def store(i, v):
            ref[pl.ds(pl.multiple_of(i * LANES, LANES), LANES), :] = v.astype(ref.dtype)
        return store

    def a_copy(k, part, c):
        return pltpu.make_async_remote_copy(
            src_ref=share_of(part, 2 * c + 1 - parity), dst_ref=buf_a.at[k, c],
            send_sem=a_send.at[k, c], recv_sem=a_recv.at[k, c],
            device_id=(r, f, partner), device_id_type=MESH,
        )

    def b_copy(k, part, i):
        target = 2 * lax.rem(chip + i, nh) + parity
        return pltpu.make_async_remote_copy(
            src_ref=share_of(part, target), dst_ref=buf_b.at[k, i],
            send_sem=b_send.at[k, i], recv_sem=b_recv.at[k, i],
            device_id=(r, f, target), device_id_type=MESH,
        )

    def start_pair(k, part):
        for i in range(nh):
            a_copy(k, part, i).start()

    def start_chips(k, part):
        for i in range(1, nh):
            c = lax.rem(chip + i, nh)
            target = 2 * c + parity
            a_copy(k, part, c).wait()

            def add(n, carry):
                at = pl.ds(pl.multiple_of(target * share + n * LANES, LANES), LANES)
                mine = part[at, :].astype(F32)
                theirs = buf_a[k, c, pl.ds(pl.multiple_of(n * LANES, LANES), LANES), :].astype(F32)
                part[at, :] = (mine + theirs).astype(BF)
                return carry

            lax.fori_loop(0, share // LANES, add, 0)
            b_copy(k, part, i).start()

    def finish_chips(k, part, base, store):
        a_copy(k, part, chip).wait()
        for i in range(1, nh):
            b_copy(k, part, i).wait()

        def add(n, carry):
            here = pl.ds(pl.multiple_of(n * LANES, LANES), LANES)
            at = pl.ds(pl.multiple_of(t * share + n * LANES, LANES), LANES)
            total = part[at, :].astype(F32) + buf_a[k, chip, here, :].astype(F32)
            for i in range(1, nh):
                total = total + buf_b[k, i, here, :].astype(F32)
            store(n, base[at, :].astype(F32) + total)
            return carry

        lax.fori_loop(0, share // LANES, add, 0)

    def c_copy(i):
        ref = share_of(x1, t)
        return pltpu.make_async_remote_copy(
            src_ref=ref, dst_ref=ref, send_sem=c_send.at[i], recv_sem=c_recv.at[i],
            device_id=(r, f, 2 * lax.rem(chip + i, nh) + parity), device_id_type=MESH,
        )

    def d_copy(i):
        ref = share_of(x1, 2 * lax.rem(chip - i + nh, nh) + parity)
        return pltpu.make_async_remote_copy(
            src_ref=ref, dst_ref=ref, send_sem=d_send.at[i], recv_sem=d_recv.at[i],
            device_id=(r, f, partner), device_id_type=MESH,
        )

    def s_copy(i):
        return pltpu.make_async_remote_copy(
            src_ref=squares.at[0], dst_ref=squares.at[i], send_sem=s_send.at[i], recv_sem=s_recv.at[i],
            device_id=(r, f, lax.rem(t + i, nt)), device_id_type=MESH,
        )

    send_own(0)
    normalize(functools.partial(chunk, act), g_mix, put(h), features // LANES)

    gather(0, 1, nf)
    gather(1, 1, nf)
    finish(0)
    u_acc[...] = jnp.zeros_like(u_acc)

    def mix_in(b, carry):
        at = pl.ds(pl.multiple_of(b * rows, rows), rows)
        u_acc[...] += dot_first(b_in[b], h[at, :])
        return carry

    lax.fori_loop(0, nf, mix_in, 0)
    for i in range(channels // LANES):
        first = t * channels + i * LANES
        window = jnp.int32(2) << (first // POOL_GROUP)
        behind = window // 2
        onward = window - behind
        source = lax.broadcasted_iota(jnp.int32, (SEQ_LEN, SEQ_LEN), 0)
        place = lax.broadcasted_iota(jnp.int32, (SEQ_LEN, SEQ_LEN), 1)
        inside = jnp.logical_and(source >= place - behind, source < place + onward)
        band = jnp.where(inside, 1.0, 0.0).astype(BF)
        spot = lax.broadcasted_iota(jnp.int32, (1, SEQ_LEN), 1)
        count = (jnp.minimum(spot + onward, SEQ_LEN) - jnp.maximum(spot - behind, 0)).astype(F32)
        gain = column(scale[pl.ds(first // LANES, 1), :], SEQ_LEN)
        for s in range(tokens // SEQ_LEN):
            at = (pl.ds(i * LANES, LANES), pl.ds(s * SEQ_LEN, SEQ_LEN))
            u = u_acc[at].astype(BF)
            mean = jnp.dot(u, band, preferred_element_type=F32) / count
            pooled[at] = ((mean - u.astype(F32)) * gain).astype(BF)

    gather(2, 1, nf)
    finish(1)

    def mix_out(b, carry):
        at = pl.ds(pl.multiple_of(b * rows, rows), rows)
        part0[at, :] = jnp.dot(b_out[b], pooled[...], preferred_element_type=F32).astype(BF)
        return carry

    lax.fori_loop(0, nf, mix_out, 0)
    start_pair(0, part0)
    gather(3, 1, nf)
    start_chips(0, part0)
    gather(4, 1, nf)

    def keep_x1(n, v):
        at = pl.ds(pl.multiple_of(t * share + n * LANES, LANES), LANES)
        x1[at, :] = v.astype(BF)

    finish_chips(0, part0, act, keep_x1)
    for i in range(1, nh):
        c_copy(i).start()
    d_copy(0).start()
    gather(5, 1, nf)
    for i in range(1, nh):
        c_copy(i).wait()
        d_copy(i).start()
    gather(6, 1, nf)
    for i in range(nh):
        d_copy(i).wait()
    normalize(functools.partial(chunk, x1), g_ffn, put(h), features // LANES)
    finish(2)
    finish(3)
    gate_acc[...] = jnp.zeros_like(gate_acc)
    up_acc[...] = jnp.zeros_like(up_acc)

    def project(source, acc):
        def one(b, carry):
            at = pl.ds(pl.multiple_of(b * rows, rows), rows)
            acc[...] += dot_first(source[b], h[at, :])
            return carry

        lax.fori_loop(0, nf, one, 0)

    gather(7, 1, nf)
    project(b_gate, gate_acc)
    finish(4)
    finish(5)
    project(b_up, up_acc)
    step = 32

    def activate(n, carry):
        at = pl.ds(pl.multiple_of(n * step, step), step)
        v = gate_acc[at, :]
        hidden[at, :] = (v / (1.0 + jnp.exp(-v)) * up_acc[at, :]).astype(BF)
        return carry

    lax.fori_loop(0, ff // step, activate, 0)
    finish(6)
    finish(7)

    def mlp_out(b, carry):
        at = pl.ds(pl.multiple_of(b * rows, rows), rows)
        part1[at, :] = jnp.dot(b_down[b], hidden[...], preferred_element_type=F32).astype(BF)
        return carry

    if share % rows == 0:
        blocks = share // rows

        def pair_out(c):
            theirs, ours = 2 * c + 1 - parity, 2 * c + parity
            lax.fori_loop(theirs * blocks, (theirs + 1) * blocks, mlp_out, 0)
            a_copy(1, part1, c).start()
            lax.fori_loop(ours * blocks, (ours + 1) * blocks, mlp_out, 0)

        for i in range(1, nh):
            pair_out(lax.rem(chip + i, nh))
        start_chips(1, part1)
        pair_out(chip)
    else:
        lax.fori_loop(0, nf, mlp_out, 0)
        start_pair(1, part1)
        start_chips(1, part1)
    for m in range(len(items)):
        drain(m)
    finish_chips(1, part1, x1, put(own_x))

    def square(i, total):
        v = chunk(own_x, i)
        return total + jnp.sum(v * v, axis=0, keepdims=True)

    mine = lax.fori_loop(0, share // LANES, square, jnp.zeros((1, tokens), F32))
    squares[0] = jnp.broadcast_to(mine, squares.shape[1:])
    for i in range(1, nt):
        s_copy(i).start()
    for i in range(1, nt):
        s_copy(i).wait()
    total = squares[0, pl.ds(0, 1), :]
    for i in range(1, nt):
        total = total + squares[i, pl.ds(0, 1), :]
    factor = lax.rsqrt(total / features + EPS)

    def closing(i, carry):
        gain = column(g_out[pl.ds(t * (share // LANES) + i, 1), :], tokens)
        put(out)(i, chunk(own_x, i) * factor * gain)
        return carry

    lax.fori_loop(0, share // LANES, closing, 0)


def staged(
    nr, nf, nt,
    act, w_in, w_out, w_gate, w_up, w_down, scale, g_mix, g_ffn, g_out, out,
    b_in, b_out, b_gate, b_up, b_down,
    x0, h, x1, part, pooled, gate_acc, up_acc, hidden, own_x, squares, power,
    buf_a, buf_b, back, home,
    own_sem, act_sem, in_send, out_send, zrecv, wrecv, ysend, yrecv, v_send, v_recv,
    a_send, a_recv, b_send, b_recv, c_send, c_recv, d_send, d_recv,
    e_send, e_recv, g_send, g_recv, s_send, s_recv,
):
    r, f, t = lax.axis_index("rep"), lax.axis_index("fs"), lax.axis_index("tp")
    features, tokens = act.shape
    shards = (w_in, w_out, w_gate, w_up, w_down)
    full = (b_in, b_out, b_gate, b_up, b_down)
    rows, channels = w_in.shape
    ff = w_gate.shape[0]
    share = features // nt
    nh = nt // 2
    nq = share // LANES
    chip, parity = t // 2, lax.rem(t, 2)
    partner = t + 1 - 2 * parity
    other_rep = lax.rem(r + 1, nr)
    cuts = 2
    slab = share // cuts
    items = [(0, 0), (0, 1), (1, 0), (1, 1), (2, 0), (3, 0), (2, 1), (3, 1), (4, 0), (4, 1)]
    early = 4
    extra = 7
    last = len(items)
    left = f < nf // 2
    inner = jnp.logical_and(f >= 1, f < nf - 1)
    outer = jnp.logical_not(inner)
    mate = jnp.where(left, 1 - f, 2 * nf - 3 - f)
    inward = jnp.where(left, f + 1, f - 1)
    over = jnp.where(inner, nf - 1 - f, nf - 1 - mate)
    far = jnp.where(inner, nf - 1 - mate, nf - 1 - f)
    blocks = (mate, over, far)

    own = [pltpu.make_async_copy(shards[m], full[m].at[f], own_sem.at[m]) for m in range(5)]
    stream = [pltpu.make_async_copy(act, x0, act_sem.at[0])]
    own[0].start()
    own[1].start()
    for copy in stream:
        copy.start()
    for copy in own[2:]:
        copy.start()

    barrier = pltpu.get_barrier_semaphore()
    for step in (1, nf - 1):
        pl.semaphore_signal(barrier, inc=1, device_id=(r, lax.rem(f + step, nf), t), device_id_type=MESH)
    pl.semaphore_signal(barrier, inc=1, device_id=(other_rep, f, t), device_id_type=MESH)
    for i in range(1, nt):
        pl.semaphore_signal(barrier, inc=1, device_id=(r, f, lax.rem(t + i, nt)), device_id_type=MESH)
    pl.semaphore_wait(barrier, 3 + (nt - 1))

    def line(start, size=LANES):
        return pl.ds(pl.multiple_of(start, size), size)

    def part_of(m, blk, of):
        matrix, s = items[m]
        if matrix < 2:
            size = rows // cuts // nr
            return full[matrix].at[blk, line((s * nr + of) * size, size), :]
        if matrix < 4:
            size = ff // cuts // nr
            return full[matrix].at[blk, line((s * nr + of) * size, size), :]
        size = rows // cuts // nr
        return full[matrix].at[blk, :, line((s * nr + of) * size, size)]

    def remote(ref, dst, send, recv, device):
        return pltpu.make_async_remote_copy(
            src_ref=ref, dst_ref=dst, send_sem=send, recv_sem=recv, device_id=device, device_id_type=MESH
        )

    def group(m):
        return max(items[m][0] - 1, 0)

    def in_copy(m, blk, d):
        ref = part_of(m, blk, r)
        place = jnp.where(inner, 1, 0) if d == 0 else 2
        return remote(ref, ref, in_send.at[group(m)], zrecv.at[m, place], (r, inward, t))

    def out_copy(m, blk, j):
        ref = part_of(m, blk, r)
        return remote(ref, ref, out_send.at[0], zrecv.at[m, j], (r, mate, t))

    def arrive(m, j):
        ref = part_of(m, blocks[j], r)
        remote(ref, ref, in_send.at[group(m)], zrecv.at[m, j], (r, mate, t)).wait_recv()

    def lot(m):
        return (m - early) // 2 if m < 2 * cuts + early else m - early - cuts

    def w_copy(m, blk):
        ref = part_of(m, blk, other_rep)
        return remote(ref, ref, in_send.at[group(m)], wrecv.at[lot(m)], (r, mate, t))

    def v_copy(blk):
        ref = part_of(extra, blk, other_rep)
        return remote(ref, ref, v_send.at[0], v_recv.at[0], (r, inward, t))

    def y_copy(m, j, of):
        ref = part_of(m, blocks[j], of)
        place = m // 2 if m < last - 2 else last // 2 + 2 * (m - last + 2) + j - 2
        if items[m][0] == 1 and j == 0:
            place = last - 2
        return remote(ref, ref, ysend.at[group(m)], yrecv.at[place], (other_rep, f, t))

    def y_lot(ref, place):
        return remote(ref, ref, ysend.at[0], yrecv.at[place], (other_rep, f, t))

    def own_ready(m):
        if items[m][1] == 0:
            own[items[m][0]].wait()

    def send_mixer(m):
        own_ready(m)
        in_copy(m, f, 0).start()

        @pl.when(inner)
        def _():
            out_copy(m, f, 0).start()

    def hop(m, j):
        arrive(m, j)
        if j == 0:
            in_copy(m, mate, 1).start()
        else:
            out_copy(m, blocks[j], j).start()

    def side(m, j):
        y_copy(m, j, r).start()

    def relay(m, j):
        hop(m, j)
        side(m, j)

    def collect(m, j):
        arrive(m, j)
        side(m, j)

    def y_arrival(m, j):
        y_copy(m, j, other_rep).wait_recv()

    def finish(matrix, count, place):
        y_lot(full[matrix].at[pl.ds(0, count), pl.ds(0, rows // nr)], place).wait_recv()

    def send_inner(m):
        in_copy(m, f, 0).start()

    def send_outer(m):
        in_copy(m, f, 0).start()
        w_copy(m, f).start()

    def pass_on(m):
        hop(m, 0)

    def cross(m, *some):
        for j in some:
            arrive(m, j)
            if m != extra or j == 2:
                side(m, j)

    def settle(s):
        ref = full[2].at[0, pl.ds(0, ff // cuts)]
        remote(ref, ref, in_send.at[1], wrecv.at[s], (r, mate, t)).wait_recv()
        pieces = 2 * nr - (s == cuts - 1)
        y_lot(full[2].at[0, pl.ds(0, pieces * (ff // cuts // nr))], 2 + s).wait_recv()
        if s == cuts - 1:
            v_copy(over).wait_recv()

    def spot(target, q, size=LANES):
        return line(target * share + q * size, size)

    def normalize(load, gain, store, count):
        def square(i, total):
            v = load(i)
            return total + jnp.sum(v * v, axis=0, keepdims=True)

        total = lax.fori_loop(0, count, square, jnp.zeros((1, tokens), F32))
        factor = lax.rsqrt(total / features + EPS)

        def scaled(i, carry):
            store(i, load(i) * factor * column(gain[pl.ds(i, 1), :], tokens))
            return carry

        lax.fori_loop(0, count, scaled, 0)

    def chunk(ref, i):
        return ref[line(i * LANES), :].astype(F32)

    def put(ref):
        def store(i, v):
            ref[line(i * LANES), :] = v.astype(ref.dtype)
        return store

    def a_copy(k, target, q, size):
        return remote(
            part.at[k, spot(target, q, size)], buf_a.at[k, target // 2, line(q * size, size)],
            a_send.at[k], a_recv.at[k, target // 2, q], (r, f, partner),
        )

    def b_copy(k, i, q, size):
        target = 2 * lax.rem(chip + i, nh) + parity
        return remote(
            part.at[k, spot(target, q, size)], buf_b.at[k, i, line(q * size, size)],
            b_send.at[k], b_recv.at[k, i - 1, q], (r, f, target),
        )

    def c_copy(k, i, q):
        ref = x1.at[k, spot(t, q)]
        device = (r, f, 2 * lax.rem(chip + i, nh) + parity)
        return remote(ref, ref, c_send.at[k], c_recv.at[k, i - 1, q], device)

    def d_copy(k, i, q):
        ref = x1.at[k, spot(2 * lax.rem(chip - i + nh, nh) + parity, q)]
        return remote(ref, ref, d_send.at[k], d_recv.at[k, i], (r, f, partner))

    def e_copy(q):
        return remote(x1.at[0, spot(t, q)], x1.at[1, spot(t, q)], e_send.at[0], e_recv.at[q], (r, mate, t))

    def g_copy(q):
        return remote(back.at[line(q * LANES)], home.at[line(q * LANES)], g_send.at[0], g_recv.at[q], (r, mate, t))

    def s_copy(i):
        return remote(squares.at[0], squares.at[i], s_send.at[0], s_recv.at[0], (r, f, lax.rem(t + i, nt)))

    def add_pair(k, target, q, size):
        for n in range(size // LANES):
            here = line(q * size + n * LANES)
            at = line(target * share + q * size + n * LANES)
            mine, theirs = part[k, at, :].astype(F32), buf_a[k, target // 2, here, :].astype(F32)
            part[k, at, :] = (mine + theirs).astype(BF)

    def total_of(k, q):
        here = line(q * LANES)
        total = part[k, spot(t, q), :].astype(F32) + buf_a[k, chip, here, :].astype(F32)
        for i in range(1, nh):
            total = total + buf_b[k, i, here, :].astype(F32)
        return total

    send_mixer(0)
    send_mixer(1)
    for m in (2, 4, 5, 8):
        own_ready(m)

    @pl.when(outer)
    def _():
        for m in (2, 3):
            in_copy(m, f, 0).start()
        for m in (4, 5, 6):
            send_outer(m)
        send_outer(7)

    @pl.when(inner)
    def _():
        in_copy(2, f, 0).start()

    for copy in stream:
        copy.wait()
    normalize(functools.partial(chunk, x0), g_mix, put(h.at[0]), features // LANES)

    @pl.when(inner)
    def _():
        relay(0, 0)
        relay(0, 1)
        relay(1, 0)
        relay(1, 1)
        in_copy(3, f, 0).start()
        hop(2, 0)
        hop(3, 0)
        send_inner(4)
        relay(0, 2)
        relay(1, 2)
        relay(2, 1)
        relay(3, 1)
        pass_on(4)
        send_inner(5)

    @pl.when(outer)
    def _():
        for j in range(3):
            collect(0, j)
            collect(1, j)

    finish(0, nf - 1, 0)

    u_mix = dot_first(b_in[0], h[0, pl.ds(0, rows), :])
    for b in range(1, nf):
        u_mix += dot_first(b_in[b], h[0, pl.ds(b * rows, rows), :])
    gate_acc[pl.ds(0, channels), :] = u_mix
    for i in range(channels // LANES):
        first = t * channels + i * LANES
        window = jnp.int32(2) << (first // POOL_GROUP)
        behind = window // 2
        onward = window - behind
        source = lax.broadcasted_iota(jnp.int32, (SEQ_LEN, SEQ_LEN), 0)
        place = lax.broadcasted_iota(jnp.int32, (SEQ_LEN, SEQ_LEN), 1)
        inside = jnp.logical_and(source >= place - behind, source < place + onward)
        band = jnp.where(inside, 1.0, 0.0).astype(BF)
        seat = lax.broadcasted_iota(jnp.int32, (1, SEQ_LEN), 1)
        count = (jnp.minimum(seat + onward, SEQ_LEN) - jnp.maximum(seat - behind, 0)).astype(F32)
        gain = column(scale[pl.ds(first // LANES, 1), :], SEQ_LEN)
        for s in range(tokens // SEQ_LEN):
            at = (pl.ds(i * LANES, LANES), pl.ds(s * SEQ_LEN, SEQ_LEN))
            u = gate_acc[at].astype(BF)
            mean = jnp.dot(u, band, preferred_element_type=F32) / count
            pooled[at] = ((mean - u.astype(F32)) * gain).astype(BF)

    mixed = True

    def mix_out(target):
        part[0, line(target * share, share), :] = jnp.dot(
            b_out[target], pooled[...], preferred_element_type=F32
        ).astype(BF)

        @pl.when(lax.rem(target, 2) != parity)
        def _():
            a_copy(0, target, 0, share).start()

    def reduce_pair(target):
        @pl.when(lax.rem(target, 2) == parity)
        def _():
            a_copy(0, target, 0, share).wait_recv()
            for i in range(1, nh):
                @pl.when(target // 2 == lax.rem(chip + i, nh))
                def _():
                    for q in range(nq):
                        add_pair(0, target, q, LANES)
                        b_copy(0, i, q, LANES).start()

    mix_out(f)

    @pl.when(inner)
    def _():
        relay(2, 2)
        relay(3, 2)
        side(2, 0)
        side(3, 0)
        for m in (2, 3):
            out_copy(m, f, 0).start()

    reduce_pair(f)

    @pl.when(inner)
    def _():
        cross(4, 1)
        pass_on(5)
        send_inner(6)

    @pl.when(outer)
    def _():
        for j in (1, 2):
            collect(2, j)
            collect(3, j)
        collect(2, 0)
        collect(3, 0)

    finish(1, 2, 1)
    mix_out(over)
    mix_out(far)
    reduce_pair(over)
    reduce_pair(far)

    @pl.when(inner)
    def _():
        cross(4, 2)

    finish(1, 1, last - 2)
    mix_out(mate)
    reduce_pair(mate)

    @pl.when(inner)
    def _():
        cross(5, 1)

    def prepare(k, target, q):
        at = spot(target, q)
        v = x1[k, at, :].astype(F32)
        h[k, at, :] = (v * column(g_ffn[pl.ds(target * nq + q, 1), :], tokens)).astype(BF)
        power[k] += jnp.sum((v * v).reshape(LANES // 8, 8, tokens), axis=0)

    power[...] = jnp.zeros_like(power)

    for q in range(nq):
        for i in range(1, nh):
            b_copy(0, i, q, LANES).wait_recv()
        x1[0, spot(t, q), :] = (x0[spot(t, q), :].astype(F32) + total_of(0, q)).astype(BF)

        @pl.when(inner)
        def _():
            for i in range(1, nh):
                c_copy(0, i, q).start()
            d_copy(0, 0, q).start()
            prepare(0, t, q)
            if q == 0:
                pass_on(6)
                send_inner(7)
                cross(5, 2)
            if q == 1:
                cross(6, 1)
            if q == 2:
                pass_on(7)
                v_copy(f).start()
                send_inner(8)
                send_inner(9)

        @pl.when(outer)
        def _():
            e_copy(q).start()

    cut = ff // cuts
    step = 32
    wide = 2 * LANES

    def project(k, s, targets, fresh):
        at = pl.ds(s * cut, cut)
        for source, acc in ((b_gate, gate_acc), (b_up, up_acc)):
            def tokens_at(n, carry):
                here = line(n * wide, wide)
                terms = [
                    jnp.dot(source[b, at, :], h[k, line(b * rows, rows), here], preferred_element_type=F32)
                    for b in targets
                ]
                total = functools.reduce(lambda x, y: x + y, terms)
                acc[at, here] = total if fresh else acc[at, here] + total
                return carry

            lax.fori_loop(0, tokens // wide, tokens_at, 0)

    def activate(k, s):
        total = jnp.sum(power[k], axis=0, keepdims=True)
        factor = lax.rsqrt(total / features + EPS)

        def some(n, carry):
            here = line(s * cut + n * step, step)
            v = gate_acc[here, :] * factor
            hidden[k, here, :] = (v / (1.0 + jnp.exp(-v)) * (up_acc[here, :] * factor)).astype(BF)
            return carry

        lax.fori_loop(0, cut // step, some, 0)

    def mlp_out(k, target, s):
        at = spot(target, s, slab)
        part[1 + k, at, :] = dot_first(b_down[target, :, line(s * slab, slab)], hidden[k]).astype(BF)

        @pl.when(lax.rem(target, 2) != parity)
        def _():
            a_copy(1 + k, target, s, slab).start()

    def pair_up(k, target, s):
        @pl.when(lax.rem(target, 2) == parity)
        def _():
            a_copy(1 + k, target, s, slab).wait_recv()
            for i in range(1, nh):
                @pl.when(target // 2 == lax.rem(chip + i, nh))
                def _():
                    add_pair(1 + k, target, s, slab)
                    b_copy(1 + k, i, s, slab).start()

    plans = (
        [(1, 2, 0), (1, 2, 1), (1, 0, 0), (1, 0, 1), (1, 3, 0), (1, 1, 0), (1, 3, 1), (1, 1, 1),
         (0, 2, 1), (0, 3, 0), (0, 3, 1), (0, 0, 0), (0, 0, 1), (0, 1, 0), (0, 1, 1)],
        [(1, 0, 0), (1, 0, 1), (1, 1, 0), (1, 2, 0), (1, 2, 1), (1, 1, 1), (1, 3, 0), (1, 3, 1),
         (0, 0, 1), (0, 1, 0), (0, 1, 1), (0, 2, 0), (0, 3, 0), (0, 2, 1), (0, 3, 1)],
    )
    soon = jnp.logical_or(t == f, t == over)
    near = chip == f // 2

    def planned(n):
        k, s, target = jnp.int32(0), jnp.int32(0), f
        for plan, taken in zip(plans, (near, jnp.logical_not(near))):
            for at, (kk, code, ss) in enumerate(plan):
                here = jnp.logical_and(n == at, taken)
                k = jnp.where(here, kk, k)
                s = jnp.where(here, ss, s)
                target = jnp.where(here, (f, mate, over, far)[code], target)
        return k, target, s

    def give_back(s):
        for i in range(1, nh):
            b_copy(2, i, s, slab).wait_recv()
        for n in range(slab // LANES):
            q = s * (slab // LANES) + n
            back[pl.ds(q * LANES, LANES), :] = total_of(2, q).astype(BF)
            g_copy(q).start()

    def spread(q):
        e_copy(q).wait_recv()
        for i in range(1, nh):
            c_copy(1, i, q).start()
        d_copy(1, 0, q).start()
        prepare(1, t, q)

    def mine(i):
        return 2 * lax.rem(chip - i + nh, nh) + parity

    def theirs(i):
        return 2 * lax.rem(chip - i + nh, nh) + 1 - parity

    def hand_over(k, q):
        for i in range(1, nh):
            c_copy(k, i, q).wait_recv()
            d_copy(k, i, q).start()
            prepare(k, mine(i), q)

    def absorb(k, i):
        ref = x1.at[k, line(theirs(i) * share, share)]
        remote(ref, ref, d_send.at[k], d_recv.at[k, i], (r, f, partner)).wait_recv()
        for q in range(nq):
            prepare(k, theirs(i), q)

    here_blocks = (t, partner)
    away_blocks = tuple(b for i in range(1, nh) for b in (mine(i), theirs(i)))

    @pl.when(inner)
    def _():
        cross(6, 2)
        absorb(0, 0)
        hand_over(0, 0)
        settle(0)
        project(0, 0, here_blocks, True)
        cross(7, 1)
        hand_over(0, 1)
        spread(0)
        cross(7, 2)
        hand_over(0, 2)
        spread(1)
        hand_over(0, 3)
        spread(2)
        for i in range(1, nh):
            absorb(0, i)
        project(0, 0, away_blocks, False)
        activate(0, 0)
        spread(3)
        hand_over(1, 0)
        absorb(1, 0)
        project(1, 0, here_blocks, True)
        cross(8, 1)
        pass_on(8)
        hand_over(1, 1)
        settle(1)
        project(0, 1, here_blocks + away_blocks, True)
        activate(0, 1)
        hand_over(1, 2)
        pass_on(9)
        project(1, 1, here_blocks, True)
        cross(9, 1)

        @pl.when(near)
        def _():
            y_arrival(8, 1)

        lead = jnp.where(near, over, f)
        mlp_out(0, lead, 0)
        hand_over(1, 3)
        for i in range(1, nh):
            absorb(1, i)
        cross(8, 2)
        pair_up(0, lead, 0)
        project(1, 0, away_blocks, False)
        activate(1, 0)
        project(1, 1, away_blocks, False)
        cross(9, 2)
        activate(1, 1)

        def ffn(n, carry):
            near_waits = (
                (1, lambda: y_arrival(9, 1)),
                (4, lambda: y_arrival(8, 2)),
                (5, lambda: w_copy(8, mate).wait_recv()),
                (6, lambda: y_arrival(9, 2)),
                (7, lambda: w_copy(9, mate).wait_recv()),
            )
            away_waits = (
                (2, lambda: w_copy(8, mate).wait_recv()),
                (3, lambda: y_arrival(8, 1)),
                (4, lambda: y_arrival(9, 1)),
                (5, lambda: w_copy(9, mate).wait_recv()),
                (6, lambda: y_arrival(8, 2)),
                (7, lambda: y_arrival(9, 2)),
            )
            for waits, taken in ((near_waits, near), (away_waits, jnp.logical_not(near))):
                for at, wait in waits:
                    @pl.when(jnp.logical_and(n == at, taken))
                    def _():
                        wait()

            mlp_out(*planned(n))

            @pl.when(n >= 1)
            def _():
                pair_up(*planned(n - 1))

            for s, first, second in ((0, 8, 10), (1, 9, 13)):
                @pl.when(n == jnp.where(soon, first, second))
                def _():
                    give_back(s)

            return carry

        lax.fori_loop(0, len(plans[0]), ffn, 0)
        pair_up(*planned(len(plans[0]) - 1))
        for q in range(nq):
            for i in range(1, nh):
                if q % (slab // LANES) == 0:
                    b_copy(1, i, q // (slab // LANES), slab).wait_recv()
            own_x[pl.ds(q * LANES, LANES), :] = x1[0, spot(t, q), :].astype(F32) + total_of(1, q)

    @pl.when(outer)
    def _():
        for m in (8, 9):
            in_copy(m, f, 0).start()
        for m in (8, 9):
            w_copy(m, f).start()
        for q in range(nq):
            g_copy(q).wait_recv()
            at = pl.ds(q * LANES, LANES)
            own_x[at, :] = x1[0, spot(t, q), :].astype(F32) + home[at, :].astype(F32)

    total = jnp.zeros((1, tokens), F32)
    for q in range(nq):
        v = own_x[pl.ds(q * LANES, LANES), :]
        total += jnp.sum(v * v, axis=0, keepdims=True)
    squares[0] = jnp.broadcast_to(total, squares.shape[1:])
    for i in range(1, nt):
        s_copy(i).start()

    got = squares.at[pl.ds(1, nt - 1)]
    remote(got, got, s_send.at[0], s_recv.at[0], (r, f, partner)).wait_recv()
    for i in range(1, nt):
        total = total + squares[i, pl.ds(0, 1), :]
    factor = lax.rsqrt(total / features + EPS)

    def closing(q):
        gain = column(g_out[pl.ds(t * nq + q, 1), :], tokens)
        out[pl.ds(q * LANES, LANES), :] = (own_x[pl.ds(q * LANES, LANES), :] * factor * gain).astype(BF)

    for q in range(nq):
        closing(q)

    def sent(ref, sem):
        remote(ref, ref, sem, zrecv.at[0, 0], (r, mate, t)).wait_send()

    for matrix in (2, 3, 4):
        sent(full[matrix].at[0], in_send.at[matrix - 1])
    sent(full[0].at[pl.ds(0, nf - 1)], ysend.at[0])
    sent(part.at[0, pl.ds(0, nh * share)], a_send.at[0])
    sent(part.at[0, pl.ds(0, (nh - 1) * share)], b_send.at[0])
    sent(squares.at[pl.ds(1, nt - 1)], s_send.at[0])

    @pl.when(inner)
    def _():
        sent(full[0].at[pl.ds(0, 2)], in_send.at[0])
        sent(full[0].at[pl.ds(0, nf - 1)], out_send.at[0])
        v_copy(f).wait_send()
        sent(full[2].at[0], ysend.at[1])
        sent(full[3].at[0, pl.ds(0, (2 * nr - 1) * (ff // cuts // nr))], ysend.at[2])
        sent(full[4].at[0], ysend.at[3])
        for k in (0, 1):
            sent(part.at[0, pl.ds(0, nh * share)], a_send.at[1 + k])
            sent(part.at[0, pl.ds(0, (nh - 1) * share)], b_send.at[1 + k])
            sent(part.at[0, pl.ds(0, nh * share)], d_send.at[k])
            sent(part.at[0, pl.ds(0, (nh - 1) * share)], c_send.at[k])
        sent(back, g_send.at[0])

    @pl.when(outer)
    def _():
        sent(full[0].at[0], in_send.at[0])
        sent(back, e_send.at[0])


def solution(mesh):
    nr, nf, nt = mesh.shape["rep"], mesh.shape["fs"], mesh.shape["tp"]

    def staged_call(act, w_in, w_out, w_gate, w_up, w_down, scale, g_mix, g_ffn, g_out):
        features, tokens = act.shape
        rows, channels = w_in.shape
        ff = w_gate.shape[1]
        share = features // nt
        nh = nt // 2
        nq = share // LANES
        anywhere = pl.BlockSpec(memory_space=pl.ANY)
        vmem = pl.BlockSpec(memory_space=pltpu.VMEM)
        dma = pltpu.SemaphoreType.DMA
        scratch = [
            pltpu.VMEM((nf, rows, channels), BF),
            pltpu.VMEM((nf, rows, channels), BF),
            pltpu.VMEM((nf, ff, rows), BF),
            pltpu.VMEM((nf, ff, rows), BF),
            pltpu.VMEM((nf, ff, rows), BF),
            pltpu.VMEM((features, tokens), BF),
            pltpu.VMEM((2, features, tokens), BF),
            pltpu.VMEM((2, features, tokens), BF),
            pltpu.VMEM((3, features, tokens), BF),
            pltpu.VMEM((channels, tokens), BF),
            pltpu.VMEM((ff, tokens), F32),
            pltpu.VMEM((ff, tokens), F32),
            pltpu.VMEM((2, ff, tokens), BF),
            pltpu.VMEM((share, tokens), F32),
            pltpu.VMEM((nt, 8, tokens), F32),
            pltpu.VMEM((2, 8, tokens), F32),
            pltpu.VMEM((3, nh, share, tokens), BF),
            pltpu.VMEM((3, nh, share, tokens), BF),
            pltpu.VMEM((share, tokens), BF),
            pltpu.VMEM((share, tokens), BF),
            dma((5,)), dma((1,)),
            dma((4,)), dma((1,)), dma((10, 3)), dma((4,)), dma((4,)), dma((9,)), dma((1,)), dma((1,)),
            dma((3,)), dma((3, nh, 2)), dma((3,)), dma((3, nh - 1, nq)),
            dma((2,)), dma((2, nh - 1, nq)), dma((2,)), dma((2, nh)),
            dma((1,)), dma((nq,)), dma((1,)), dma((nq,)), dma((1,)), dma((1,)),
        ]
        return pl.pallas_call(
            functools.partial(staged, nr, nf, nt),
            out_shape=jax.ShapeDtypeStruct((share, tokens), BF),
            in_specs=[anywhere] * 6 + [vmem] * 4,
            out_specs=vmem,
            scratch_shapes=scratch,
            compiler_params=pltpu.CompilerParams(
                collective_id=0, has_side_effects=True, vmem_limit_bytes=60 * 1024 * 1024
            ),
        )(
            act, w_in, w_out, w_gate.T, w_up.T, w_down.T,
            *[v.reshape(-1, LANES) for v in (scale, g_mix, g_ffn, g_out)],
        )

    def on_device(act, w_in, w_out, w_gate, w_up, w_down, scale, g_mix, g_ffn, g_out):
        features, tokens = act.shape
        rows, channels = w_in.shape
        ff = w_gate.shape[1]
        share = features // nt
        nh = nt // 2
        if nr == 2 and nf == 4 and share == rows and rows % (2 * nr * LANES) == 0 and ff % (32 * nr) == 0:
            return staged_call(act, w_in, w_out, w_gate, w_up, w_down, scale, g_mix, g_ffn, g_out)
        anywhere = pl.BlockSpec(memory_space=pl.ANY)
        vmem = pl.BlockSpec(memory_space=pltpu.VMEM)
        dma = pltpu.SemaphoreType.DMA
        scratch = [
            pltpu.VMEM((nf, rows, channels), BF),
            pltpu.VMEM((nf, rows, channels), BF),
            pltpu.VMEM((nf, rows, ff), BF),
            pltpu.VMEM((nf, rows, ff), BF),
            pltpu.VMEM((nf, rows, ff), BF),
            pltpu.VMEM((features, tokens), BF),
            pltpu.VMEM((features, tokens), BF),
            pltpu.VMEM((features, tokens), BF),
            pltpu.VMEM((features, tokens), BF),
            pltpu.VMEM((channels, tokens), F32),
            pltpu.VMEM((channels, tokens), BF),
            pltpu.VMEM((ff, tokens), F32),
            pltpu.VMEM((ff, tokens), F32),
            pltpu.VMEM((ff, tokens), BF),
            pltpu.VMEM((share, tokens), F32),
            pltpu.VMEM((nt, 8, tokens), F32),
            pltpu.VMEM((2, nh, share, tokens), BF),
            pltpu.VMEM((2, nh, share, tokens), BF),
            dma((5,)),
            dma((8, 2, 2)),
            dma((8, nf)),
            dma((8, 2, 2, max(nr - 1, 1))),
            dma((8, nf, max(nr - 1, 1))),
            dma((2, nh)), dma((2, nh)), dma((2, nh)), dma((2, nh)),
            dma((nh,)), dma((nh,)), dma((nh,)), dma((nh,)),
            dma((nt,)), dma((nt,)),
        ]
        return pl.pallas_call(
            functools.partial(body, nr, nf, nt),
            out_shape=jax.ShapeDtypeStruct((share, tokens), BF),
            in_specs=[vmem] + [anywhere] * 5 + [vmem] * 4,
            out_specs=vmem,
            scratch_shapes=scratch,
            compiler_params=pltpu.CompilerParams(
                collective_id=0, has_side_effects=True, vmem_limit_bytes=60 * 1024 * 1024
            ),
        )(
            act, w_in, w_out, w_gate, w_up, w_down,
            *[v.reshape(-1, LANES) for v in (scale, g_mix, g_ffn, g_out)],
        )

    weight = P("fs", "tp")
    tokens_split = P(None, ("rep", "fs"))
    return jax.shard_map(
        on_device,
        mesh=mesh,
        in_specs=(tokens_split, *[weight] * 5, P(), P(), P(), P()),
        out_specs=P("tp", ("rep", "fs")),
        check_vma=False,
    )
```
